256 devices in a mesh: sp: 16 (over y, x), tp: 16 (over z, core).
Axes of the slice: x: 4, y: 4, z: 8, core: 2. Of those that a mesh axis runs over, the one named last changes fastest.
Arguments:
- queries: bfloat16 [16384, 1024], P('sp', 'tp'), may hold values from -18 to 18
- keys: bfloat16 [16384, 256], P('sp'), may hold values from -18 to 18
- values: bfloat16 [16384, 256], P('sp'), may hold values from -6 to 6
- sink_logits: float32 [16], P('tp'), may hold values from 3 to 7
- w_out: bfloat16 [1024, 2048], P('tp'), may hold values from -1.5 to 1.5
- residual: bfloat16 [16384, 2048], P(('sp', 'tp')), may hold values from -6 to 6
- norm_gain: float32 [2048], replicated, may hold values from 0.1 to 1.9
- expert_ids: int32 [16384, 4], P('sp'), may hold values from 0 to 127, all different within a row; in each aligned block of 1024 rows (0 to 1023, 1024 to 2047, ...) at most 64 rows name the same one
- expert_weights: float32 [16384, 4], P('sp'), may hold values from 0.1 to 1.5
- w_gate: bfloat16 [256, 768, 2048], P(('sp', 'tp')), may hold values from -0.125 to 0.125
- w_up: bfloat16 [256, 768, 2048], P(('sp', 'tp')), may hold values from -0.125 to 0.125
- w_down: bfloat16 [256, 768, 2048], P(('sp', 'tp')), may hold values from -0.15625 to 0.15625
- shared_gate: bfloat16 [512, 2048], P('tp'), may hold values from -0.125 to 0.125
- shared_up: bfloat16 [512, 2048], P('tp'), may hold values from -0.125 to 0.125
- shared_down: bfloat16 [512, 2048], P('tp'), may hold values from -0.25 to 0.25
Outputs:
- layer_out: bfloat16 [16384, 2048], P(('sp', 'tp'))
The draws below stay inside these ranges and needn't reach their ends.
Inputs may be any that keep to these rules, and one draw needn't show every extreme that they name: `expert_ids`: each row names 4 different experts; in each aligned block of 1024 rows no expert is named by more than 64 rows.
All inputs are finite; a program needn't handle non-finite values.
Results may differ from the reference program's by a relative error of at most 0.02.
Values may be sent and summed in bfloat16 or wider, within the bound.
A program may use at most 128 MiB of HBM per device.

```python
import math
import jax
import jax.numpy as jnp
import numpy as np
from jax import lax

D = 2048
HQ = 16
HD = 64
KVH = 4
GROUP = 4
WINDOW = 128
TOK_DEV = 1024
TOKENS = 16384
EXPERTS = 128
TOPK = 4
FF = 1536
SFF = 512
CAP = 64
N_SP = 16
N_TP = 16


def draw_queries(key, part):
    drawn = jnp.clip(jax.random.normal(jax.random.fold_in(key, 11), (TOKENS, HQ * HD), jnp.float32), -6.0, 6.0)
    return drawn.astype(jnp.bfloat16)


def draw_keys(key, part):
    drawn = jnp.clip(jax.random.normal(jax.random.fold_in(key, 23), (TOKENS, KVH * HD), jnp.float32), -6.0, 6.0)
    return drawn.astype(jnp.bfloat16)


def block_levels(key, extent, pieces, low, high):
    def one(dim, blocks):
        heights = jax.random.uniform(jax.random.fold_in(jax.random.fold_in(key, 6), dim), (blocks,), jnp.float32, low / len(pieces), high / len(pieces))
        return jnp.repeat(jnp.exp(heights), extent[dim] // blocks).reshape((-1,) + (1,) * (len(extent) - dim - 1))

    level = one(*pieces[0])
    for cut in pieces[1:]:
        level = level * one(*cut)
    return level


def shared_out(own_key, own, number, rows, count, top, most, slope):
    ranking = jax.random.permutation(own_key, count)
    crowded, common = portions_of(count, rows * top, most, slope, True), portions_of(count, rows * top, most, slope, False)
    places = jnp.arange(count)

    def named(lengths, rotation):
        used = int((lengths > 0).sum())
        fixed = max(1, used // 4)
        shifted = fixed + (places - fixed + rotation * (used - fixed)) % max(1, count - fixed)
        return jnp.zeros((count,), jnp.int32).at[ranking[jnp.where(places < fixed, places, shifted)]].set(jnp.asarray(lengths, jnp.int32))

    lengths = jnp.where(number % 4 == 0, named(crowded, number // 4), named(common, number - number // 4 - 1))
    mixed = jax.random.permutation(jax.random.fold_in(own, 3), count)
    giver, sink = mixed[0:count // 2 * 2:2], mixed[1:count // 2 * 2:2]
    room = jnp.minimum(lengths[giver] - 1, most - lengths[sink]) // 2
    room = jnp.where((giver == ranking[0]) | (sink == ranking[0]) | (lengths[sink] == 0), 0, jnp.maximum(room, 0))
    shifted = jax.random.randint(jax.random.fold_in(own, 4), (count // 2,), 0, 1 << 20) % (room + 1)
    lengths = lengths.at[giver].add(-shifted).at[sink].add(shifted)
    items = jnp.searchsorted(jnp.cumsum(lengths), jnp.arange(rows * top), side="right").astype(jnp.int32)
    listing = items.reshape(top, rows).T
    listing = listing[jax.random.permutation(jax.random.fold_in(own, 1), rows)]
    rotation = jax.random.randint(jax.random.fold_in(own, 2), (rows, 1), 0, top)
    return jnp.take_along_axis(listing, (jnp.arange(top)[None, :] + rotation) % top, axis=1)


def portions_of(amount, total, reach, skew, full):
    portions = [(1 << 20) // math.isqrt(standing ** skew) + 1 for standing in range(1, amount + 1)]
    largest = reach if full else min(reach, max(-(-total // amount), total * portions[0] // sum(portions)))
    least = 1 if total - largest >= amount - 1 else 0
    counts, spare = [largest] + [least] * (amount - 1), total - largest - least * (amount - 1)
    while spare > 0:
        candidates = [i for i in range(1, amount) if counts[i] < largest] or [i for i in range(1, amount) if counts[i] < reach]
        pool, budget = sum([portions[i] for i in candidates]), spare
        for i in candidates:
            addition = min(reach - counts[i], max(1, budget * portions[i] // pool), spare)
            counts[i] = counts[i] + addition
            spare = spare - addition
    return np.array(counts)


def normal_values(rng, shape, width, most, split=(), held_as=jnp.bfloat16):
    gain = block_levels(rng, shape, split, -0.22, 0.18) if split else 1.0
    values = jax.random.normal(rng, shape, jnp.float32) * width * gain
    return jnp.minimum(jnp.maximum(values, -most), most).astype(held_as)


def setup_inputs(seed: int = 0) -> dict:
    key_of = jax.random.split(jax.random.key(seed), 16)
    queries = draw_queries(jax.random.fold_in(key_of[15], 71), 0)
    keys = draw_keys(jax.random.fold_in(key_of[15], 71), 0)
    values = normal_values(key_of[2], (TOKENS, KVH * HD), 1.0, 6.0, ((0, 16),))
    sink_logits = jnp.clip(3.0 + 4.0 * jax.random.uniform(key_of[3], (HQ,), jnp.float32) ** block_levels(key_of[3], (HQ,), ((0, 16),), -0.2, 0.2), 3.0, 7.0)
    w_out = normal_values(key_of[4], (HQ * HD, D), (HQ * HD // 64) ** -0.5, 1.5, ((0, 16),))
    residual = normal_values(key_of[5], (TOKENS, D), 1.0, 6.0, ((0, 256),))
    norm_gain = jnp.clip(1.0 + 0.18 * jax.random.normal(key_of[6], (D,), jnp.float32), 0.1, 1.9)
    expert_ids_keys = jax.random.split(jax.random.fold_in(key_of[7], 1), TOKENS // TOK_DEV)
    expert_ids_turns = jax.random.permutation(jax.random.fold_in(key_of[7], 3), TOKENS // TOK_DEV)
    expert_ids = jax.vmap(lambda own, number: shared_out(jax.random.fold_in(key_of[7], 2), own, number, TOK_DEV, EXPERTS, TOPK, CAP, 2))(expert_ids_keys, expert_ids_turns).reshape((TOKENS, TOPK))
    expert_weights = jnp.clip(jnp.exp(math.log(1.5) - 2.7080502 * jax.random.uniform(key_of[8], (TOKENS, TOPK), jnp.float32) ** block_levels(key_of[8], (TOKENS, TOPK), ((0, 16),), -0.2, 0.2)), 0.1, 1.5)
    w_gate = normal_values(key_of[9], (2 * EXPERTS, FF // 2, D), D ** -0.5, 0.125, ((0, 256),))
    w_up = normal_values(key_of[10], (2 * EXPERTS, FF // 2, D), D ** -0.5, 0.125, ((0, 256),))
    w_down = normal_values(key_of[11], (2 * EXPERTS, FF // 2, D), FF ** -0.5, 0.15625, ((0, 256),))
    shared_gate = normal_values(key_of[12], (SFF, D), D ** -0.5, 0.125, ((0, 16),))
    shared_up = normal_values(key_of[13], (SFF, D), D ** -0.5, 0.125, ((0, 16),))
    shared_down = normal_values(key_of[14], (SFF, D), SFF ** -0.5, 0.25, ((0, 16),))
    return dict(queries=queries, keys=keys, values=values, sink_logits=sink_logits, w_out=w_out, residual=residual, norm_gain=norm_gain, expert_ids=expert_ids, expert_weights=expert_weights, w_gate=w_gate, w_up=w_up, w_down=w_down, shared_gate=shared_gate, shared_up=shared_up, shared_down=shared_down)


def attend(queries, keys, values, sink_logits):
    seq_rows = queries.shape[0]
    num_blocks = seq_rows // WINDOW
    query_blocks = queries.astype(jnp.float32).reshape(num_blocks, WINDOW, KVH, GROUP, HD)
    key_blocks = keys.astype(jnp.float32).reshape(num_blocks, WINDOW, KVH, HD)
    value_blocks = values.astype(jnp.float32).reshape(num_blocks, WINDOW, KVH, HD)

    def shift_back(blocks):
        return jnp.concatenate([jnp.zeros_like(blocks[:1]), blocks[:-1]], axis=0)
    keys_ext = jnp.concatenate([shift_back(key_blocks), key_blocks], axis=1)
    values_ext = jnp.concatenate([shift_back(value_blocks), value_blocks], axis=1)
    scores = jnp.einsum('nqhgd,nshd->nhgqs', query_blocks, keys_ext) * HD ** (-0.5)
    query_pos = jnp.arange(WINDOW)[:, None] + WINDOW
    key_pos = jnp.arange(2 * WINDOW)[None, :]
    in_band = (key_pos <= query_pos) & (key_pos > query_pos - WINDOW)
    absolute = jnp.arange(num_blocks)[:, None, None] * WINDOW + key_pos[None] - WINDOW
    allowed = in_band[None] & (absolute >= 0)
    scores = jnp.where(allowed[:, None, None], scores, -jnp.inf)
    sink_col = jnp.broadcast_to(sink_logits.reshape(KVH, GROUP)[None, :, :, None, None], scores.shape[:-1] + (1,))
    combined = jnp.concatenate([scores, sink_col], axis=-1)
    row_max = lax.optimization_barrier(jnp.max(combined, axis=-1, keepdims=True))
    exps = jnp.exp(combined - row_max)
    weights = (exps[..., :-1] / lax.optimization_barrier(jnp.sum(exps, axis=-1, keepdims=True))).astype(jnp.bfloat16)
    attended = jnp.einsum('nhgqs,nshd->nqhgd', weights.astype(jnp.float32), values_ext)
    return attended.astype(jnp.bfloat16).reshape(seq_rows, HQ * HD)

def normalize(after_mix, norm_gain):
    values_f = after_mix.astype(jnp.float32)
    scale = lax.rsqrt(lax.optimization_barrier(jnp.mean(values_f * values_f, axis=-1, keepdims=True)) + 1e-06)
    return (values_f * scale * norm_gain).astype(jnp.bfloat16)

def slot_layout(route_ids):
    flat_ids = route_ids.reshape(-1).astype(jnp.int32)
    matches = (flat_ids[:, None] == jnp.arange(EXPERTS, dtype=jnp.int32)[None, :]).astype(jnp.int32)
    earlier = jnp.cumsum(matches, axis=0).astype(jnp.int32) - matches
    order_in = lax.optimization_barrier(jnp.sum(earlier * matches, axis=1)).astype(jnp.int32)
    slot_index = flat_ids * CAP + order_in
    owners = jnp.arange(flat_ids.shape[0], dtype=jnp.int32) // TOPK
    slot_owner = jnp.full((EXPERTS * CAP,), -1, jnp.int32).at[slot_index].set(owners)
    return (slot_index, slot_owner)

def run_expert(operands):
    row_block, gate_w, up_w, down_w = operands
    total = jnp.zeros((row_block.shape[0], D), jnp.float32)
    for half in range(2):
        gate_act = jnp.dot(row_block, gate_w[half].T, preferred_element_type=jnp.float32)
        up_act = jnp.dot(row_block, up_w[half].T, preferred_element_type=jnp.float32)
        hidden = (jax.nn.silu(gate_act) * up_act).astype(jnp.bfloat16)
        term = jnp.dot(hidden, down_w[half], preferred_element_type=jnp.float32).astype(jnp.bfloat16)
        term = lax.optimization_barrier(term)
        total = total + term.astype(jnp.float32)
    return total.astype(jnp.bfloat16)

def reference(queries, keys, values, sink_logits, w_out, residual, norm_gain, expert_ids, expert_weights, w_gate, w_up, w_down, shared_gate, shared_up, shared_down):
    attended = attend(queries, keys, values, sink_logits)
    projected = jnp.dot(attended, w_out, preferred_element_type=jnp.float32)
    after_mix = (residual.astype(jnp.float32) + projected).astype(jnp.bfloat16)
    normed = normalize(after_mix, norm_gain)
    block_rows = normed.reshape(N_SP, TOK_DEV, D)
    block_ids = expert_ids.reshape(N_SP, TOK_DEV, TOPK)
    slot_index, slot_owner = jax.vmap(slot_layout)(block_ids)

    def fill_slots(rows_here, owner_here):
        picked = rows_here[jnp.maximum(owner_here, 0)]
        return jnp.where((owner_here >= 0)[:, None], picked, jnp.zeros((), jnp.bfloat16))
    slot_rows = jax.vmap(fill_slots)(block_rows, slot_owner)
    per_expert = jnp.transpose(slot_rows.reshape(N_SP, EXPERTS, CAP, D), (1, 0, 2, 3)).reshape(EXPERTS, N_SP * CAP, D)
    gate_pieces = w_gate.reshape(EXPERTS, 2, FF // 2, D)
    up_pieces = w_up.reshape(EXPERTS, 2, FF // 2, D)
    down_pieces = w_down.reshape(EXPERTS, 2, FF // 2, D)
    expert_out = lax.map(run_expert, (per_expert, gate_pieces, up_pieces, down_pieces))
    returned = jnp.transpose(expert_out.reshape(EXPERTS, N_SP, CAP, D), (1, 0, 2, 3)).reshape(N_SP, EXPERTS * CAP, D)
    shared_hidden = (jax.nn.silu(jnp.dot(normed, shared_gate.T, preferred_element_type=jnp.float32)) * jnp.dot(normed, shared_up.T, preferred_element_type=jnp.float32)).astype(jnp.bfloat16)
    lanes = N_TP // 2
    half_cap = CAP // 2
    unit_width = SFF // N_TP

    def block_moe(operands):
        outputs, index_flat, ids, wts, hidden_rows = operands
        index_pairs = index_flat.reshape(TOK_DEV, TOPK)
        rank = index_pairs - ids * CAP
        group = 2 * (ids % lanes) + rank // half_cap
        chosen = [outputs[index_pairs[:, k]].astype(jnp.float32) for k in range(TOPK)]

        def add_group(total, group_id):
            part = jnp.zeros((TOK_DEV, D), jnp.float32)
            for k in range(TOPK):
                factor = jnp.where(group[:, k] == group_id, wts[:, k], jnp.zeros((), wts.dtype))
                part = part + factor[:, None] * chosen[k]
            hid = lax.dynamic_slice_in_dim(hidden_rows, group_id * unit_width, unit_width, 1)
            down = lax.dynamic_slice_in_dim(shared_down, group_id * unit_width, unit_width, 0)
            part = part + jnp.dot(hid, down, preferred_element_type=jnp.float32)
            rounded = lax.optimization_barrier(part.astype(jnp.bfloat16))
            return (total + rounded.astype(jnp.float32), None)
        total, _ = lax.scan(add_group, jnp.zeros((TOK_DEV, D), jnp.float32), jnp.arange(N_TP, dtype=jnp.int32))
        return total.astype(jnp.bfloat16)
    moe_out = lax.map(block_moe, (returned, slot_index, block_ids, expert_weights.reshape(N_SP, TOK_DEV, TOPK), shared_hidden.reshape(N_SP, TOK_DEV, SFF)))
    moe_out = moe_out.reshape(TOKENS, D)
    return (after_mix.astype(jnp.float32) + moe_out.astype(jnp.float32)).astype(jnp.bfloat16)
```

```python
import jax
import jax.numpy as jnp
from jax import lax
from jax.experimental import pallas as pl
from jax.experimental.pallas import tpu as pltpu
from jax.sharding import PartitionSpec as P

HD = 64
GROUP = 4
WINDOW = 128
TOPK = 4


def shifted(block, axis, distance):
    devices = range(lax.axis_size(axis))
    route = [(i - distance, i) for i in devices if i - distance in devices]
    return lax.ppermute(block, axis, route)


def normalize(after_mix, norm_gain):
    values_f = after_mix.astype(jnp.float32)
    scale = lax.rsqrt(jnp.mean(values_f * values_f, axis=-1, keepdims=True) + 1e-06)
    return (values_f * scale * norm_gain).astype(jnp.bfloat16)


MESH = pl.DeviceIdType.MESH
CHUNKS = 4
CAP = 64


def dot_nt(a, b):
    return lax.dot_general(a, b, (((1,), (1,)), ((), ())), preferred_element_type=jnp.float32)


def dot_nn(a, b):
    return jnp.dot(a, b, preferred_element_type=jnp.float32)


def rows_loop(total, step, fn):
    def one(i, carry):
        fn(pl.ds(pl.multiple_of(i * step, step), step))
        return carry

    lax.fori_loop(0, total // step, one, 0)


class Place:
    def __init__(self):
        self.sp_count = lax.axis_size("sp")
        self.tp_count = lax.axis_size("tp")
        self.s = lax.axis_index("sp")
        self.t = lax.axis_index("tp")
        self.c = self.t % 2
        self.z = self.t // 2
        self.nz = self.tp_count // 2
        self.partner = (self.s, self.t + 1 - 2 * self.c)
        self.right = (self.s, (self.t + 2) % self.tp_count)
        self.left = (self.s, (self.t + self.tp_count - 2) % self.tp_count)

    def peer(self, o):
        return ((self.s + o) % self.sp_count, self.t)

    def barrier(self, devices, peers=True):
        sem = pltpu.get_barrier_semaphore()
        for device in devices:
            pl.semaphore_signal(sem, inc=1, device_id=device, device_id_type=MESH)
        count = len(devices)
        if peers:

            def one(o, carry):
                pl.semaphore_signal(sem, inc=1, device_id=self.peer(o), device_id_type=MESH)
                return carry

            lax.fori_loop(1, self.sp_count, one, 0)
            count += self.sp_count - 1
        pl.semaphore_wait(sem, count)

    def steps(self, j):
        far, near = self.nz // 2, self.nz - 1 - self.nz // 2
        return (far, near) if j % 2 == 0 else (near, far)


def remote(src, dst, send_sem, recv_sem, device):
    return pltpu.make_async_remote_copy(
        src_ref=src, dst_ref=dst, send_sem=send_sem, recv_sem=recv_sem, device_id=device, device_id_type=MESH
    )


class RingGather:
    def __init__(self, p, buf, rows, send_sems, recv_sems):
        self.p, self.buf, self.rows = p, buf, rows
        self.ss, self.rs = send_sems, recv_sems

    def copy(self, j, way, k, shift):
        p = self.p
        origin = (p.z - shift if way == 0 else p.z + shift) + p.nz
        block = self.buf.at[j, pl.ds(pl.multiple_of(origin % p.nz * self.rows, self.rows), self.rows)]
        return remote(block, block, self.ss.at[j, way, k - 1], self.rs.at[j, way, k - 1], p.left if way else p.right)

    def send(self, j, k):
        for way in range(2):
            if k <= self.p.steps(j)[way]:
                self.copy(j, way, k, k - 1).start()

    def wait(self, j, k):
        for way in range(2):
            if k <= self.p.steps(j)[way]:
                self.copy(j, way, k, k).wait_recv()

    def drain(self, j):
        for way in range(2):
            for k in range(1, self.p.steps(j)[way] + 1):
                self.copy(j, way, k, k - 1).wait_send()


class Exchange:
    def __init__(self, p, src, dst, rows, send_sems, recv_sems):
        self.p, self.src, self.dst, self.rows = p, src, dst, rows
        self.ss, self.rs = send_sems, recv_sems

    def block(self, index):
        return pl.ds(pl.multiple_of(index * self.rows, self.rows), self.rows)

    def send(self, j):
        p = self.p

        def one(o, carry):
            peer = p.peer(o)
            remote(
                self.src.at[j, self.block(peer[0])],
                self.dst.at[j, self.block(p.s)],
                self.ss.at[j],
                self.rs.at[j],
                peer,
            ).start()
            return carry

        lax.fori_loop(1, p.sp_count, one, 0)
        self.dst[j, self.block(p.s)] = self.src[j, self.block(p.s)]

    def all_of(self, j):
        others = pl.ds(0, (self.p.sp_count - 1) * self.rows)
        return remote(self.src.at[j, others], self.dst.at[j, others], self.ss.at[j], self.rs.at[j], self.p.peer(1))

    def wait(self, j):
        self.all_of(j).wait_recv()

    def drain(self, j):
        self.all_of(j).wait_send()


def dispatch_kernel(
    normed, pick, wg_hbm, wu_hbm, sg, su, hidden, shared,
    ring_buf, outgoing, own, other, wg, wu, gate_sum, up_sum, sgu, pre, pre_other,
    w_sem, x_send, x_recv, ring_send, ring_recv, a_send, a_recv, f_send, f_recv, s_send, s_recv,
):
    p = Place()
    c, nc = p.c, CHUNKS
    slots, rows = pick.shape
    my_rows, width = normed.shape
    half = width // 2
    fc = half // nc
    units = sg.shape[0]
    chip_rows = 2 * my_rows
    tile = min(256, slots)
    fetch_gate = pltpu.make_async_copy(wg_hbm, wg, w_sem.at[0])
    fetch_up = pltpu.make_async_copy(wu_hbm, wu, w_sem.at[1])
    fetch_gate.start()
    fetch_up.start()
    p.barrier([p.partner, p.right, p.left])

    mine = pl.ds(pl.multiple_of(p.z * chip_rows + c * my_rows, my_rows), my_rows)

    def cols(h, j):
        return pl.ds(pl.multiple_of(h * half + j * fc, fc), fc)

    def swap(j):
        return remote(normed.at[:, cols(1 - c, j)], ring_buf.at[j, mine], x_send.at[j], x_recv.at[j], p.partner)

    def swapped(j):
        theirs = pl.ds(pl.multiple_of(p.z * chip_rows + (1 - c) * my_rows, my_rows), my_rows)
        return remote(ring_buf.at[j, theirs], ring_buf.at[j, theirs], x_send.at[j], x_recv.at[j], p.partner)

    for j in range(nc):
        swap(j).start()
    half_cols = [pl.ds(pl.multiple_of(h * half, half), half) for h in (c, 1 - c)]
    sgu_rows = [pl.ds(pl.multiple_of(k * 2 * units + c * units, units), units) for k in range(2)]
    shared_swaps = [
        remote(ref.at[:, half_cols[1]], sgu.at[sgu_rows[k]], s_send.at[k], s_recv.at[k], p.partner)
        for k, ref in enumerate((sg, su))
    ]
    for copy in shared_swaps:
        copy.start()
    for k, ref in enumerate((sg, su)):
        sgu[sgu_rows[k]] = ref[:, half_cols[0]]
    for j in range(nc):
        ring_buf[j, mine] = normed[:, cols(c, j)]

    ring = RingGather(p, ring_buf, chip_rows, ring_send, ring_recv)
    spread = Exchange(p, outgoing, own, slots // p.sp_count, a_send, a_recv)
    last = p.nz // 2

    def forward(j):
        return remote(own.at[j], other.at[j], f_send.at[j], f_recv.at[j], p.partner)

    def begin(pair):
        for j in pair:
            swapped(j).wait_recv()
            ring.send(j, 1)

    def hop(pair, k):
        for j in pair:
            ring.wait(j, k)
            ring.send(j, k + 1)

    def select(j):
        ring.wait(j, last)

        def one(r):
            outgoing[j, r] = dot_nn(pick[r], ring_buf[j]).astype(jnp.bfloat16)

        rows_loop(slots, tile, one)
        spread.send(j)

    def shared_part(j):
        def one(r):
            part = dot_nt(ring_buf[j, r], sgu[:, j * fc : (j + 1) * fc])
            pre[r] = part if j == 0 else pre[r] + part

        rows_loop(rows, tile, one)

    def arrive(j):
        spread.wait(j)
        forward(j).start()

    def multiply(j):
        forward(j).wait_recv()

        def one(r):
            a, b = own[j, r], other[j, r]
            for w, total in ((wg, gate_sum), (wu, up_sum)):
                part = dot_nt(a, w[:, cols(c, j)]) + dot_nt(b, w[:, cols(1 - c, j)])
                total[r] = part if j == 0 else total[r] + part

        rows_loop(slots, tile, one)

    first, second = (0, 1), (2, 3)
    begin(first)
    for k in range(1, last):
        hop(first, k)
    begin(second)
    for j in first:
        select(j)
    for copy in shared_swaps:
        copy.wait_recv()
    for k in range(1, last):
        hop(second, k)
        if k <= 2:
            shared_part(first[k - 1])
    for j in first:
        if last <= j + 1:
            shared_part(j)
    select(2)
    arrive(0)
    select(3)
    for j in second:
        shared_part(j)
    swap_pre = remote(pre, pre_other, s_send.at[2], s_recv.at[2], p.partner)
    swap_pre.start()
    fetch_gate.wait()
    fetch_up.wait()
    multiply(0)
    arrive(1)
    swap_pre.wait_recv()

    def shared_one(r):
        both = pre[r] + pre_other[r]
        gate, up = both[:, : 2 * units], both[:, 2 * units :]
        shared[r] = (gate / (1.0 + jnp.exp(-gate)) * up).astype(jnp.bfloat16)

    rows_loop(rows, tile, shared_one)
    multiply(1)
    arrive(2)
    multiply(2)
    arrive(3)
    multiply(3)

    def hidden_one(r):
        gate = gate_sum[r]
        hidden[r] = (gate / (1.0 + jnp.exp(-gate)) * up_sum[r]).astype(jnp.bfloat16)

    rows_loop(slots, tile, hidden_one)
    for j in range(nc):
        swap(j).wait_send()
        ring.drain(j)
        spread.drain(j)
        forward(j).wait_send()
    for copy in shared_swaps:
        copy.wait_send()
    swap_pre.wait_send()


def combine_kernel(
    hidden, wd_hbm, blend, shared, sd, after_mix, out,
    wd, half_send, half_recv, total, held, sdh, part, red_send, red_recv, moe_send, moe_recv,
    w_sem, d_send, d_recv, h_send, h_recv, a_send, a_recv, r_send, r_recv, m_send, m_recv,
):
    p = Place()
    c, nc = p.c, CHUNKS
    rows, slots = blend.shape
    my_rows, width = after_mix.shape
    half = width // 2
    fc = half // nc
    units = sd.shape[0]
    chip_rows = 2 * my_rows
    tile = min(256, slots)
    fetch = pltpu.make_async_copy(wd_hbm, wd, w_sem.at[0])
    fetch.start()
    p.barrier([p.partner, p.right, p.left])

    def cols(h, j):
        return pl.ds(pl.multiple_of(h * half + j * fc, fc), fc)

    half_cols = [pl.ds(pl.multiple_of(h * half, half), half) for h in (c, 1 - c)]
    my_units = pl.ds(pl.multiple_of(c * units, units), units)
    swap_sd = remote(sd.at[:, half_cols[1]], sdh.at[my_units], d_send.at[0], d_recv.at[0], p.partner)
    swap_sd.start()
    sdh[my_units] = sd[:, half_cols[0]]
    fetch.wait()

    spread = Exchange(p, total, held, slots // p.sp_count, a_send, a_recv)

    def give(j):
        return remote(half_send.at[j], half_recv.at[j], h_send.at[j], h_recv.at[j], p.partner)

    def down(j):
        def theirs(r):
            half_send[j, r] = dot_nn(hidden[r], wd[:, cols(1 - c, j)]).astype(jnp.bfloat16)

        def ours(r):
            total[j, r] = dot_nn(hidden[r], wd[:, cols(c, j)]).astype(jnp.bfloat16)

        rows_loop(slots, tile, theirs)
        give(j).start()
        rows_loop(slots, tile, ours)

    def add_halves(j):
        give(j).wait_recv()

        def one(r):
            both = total[j, r].astype(jnp.float32) + half_recv[j, r].astype(jnp.float32)
            total[j, r] = both.astype(jnp.bfloat16)

        rows_loop(slots, tile, one)
        spread.send(j)

    def blend_rows(j):
        spread.wait(j)

        def one(r):
            mixed = dot_nn(blend[r], held[j])
            part[j, r] = mixed + dot_nn(shared[r], sdh[:, j * fc : (j + 1) * fc])

        rows_loop(rows, tile, one)

    def chip_block(distance):
        index = (p.z + distance + p.nz) % p.nz
        return pl.ds(pl.multiple_of(index * chip_rows, chip_rows), chip_rows)

    def red(j, way, m):
        return remote(
            red_send.at[j, way, m - 1],
            red_recv.at[j, way, m - 1],
            r_send.at[j, way, m - 1],
            r_recv.at[j, way, m - 1],
            p.left if way else p.right,
        )

    def step(j, m):
        for way in range(2):
            n = p.steps(j)[way]
            if m > n:
                continue
            distance = n - m + 1
            value = part[j, chip_block(-distance if way else distance)]
            if m > 1:
                red(j, way, m - 1).wait_recv()
                value = value + red_recv[j, way, m - 2].astype(jnp.float32)
            red_send[j, way, m - 1] = value.astype(jnp.bfloat16)
            red(j, way, m).start()

    def give_rows(j):
        return remote(moe_send.at[j], moe_recv.at[j], m_send.at[j], m_recv.at[j], p.partner)

    def finish(j):
        own_rows = pl.ds(pl.multiple_of(c * my_rows, my_rows), my_rows)
        their_rows = pl.ds(pl.multiple_of((1 - c) * my_rows, my_rows), my_rows)
        ends = []
        for way in range(2):
            n = p.steps(j)[way]
            if n:
                red(j, way, n).wait_recv()
                ends.append((way, n - 1))

        def moe(which, offset):
            base = pl.ds(pl.multiple_of(p.z * chip_rows + offset * my_rows, my_rows), my_rows)
            value = part[j, base]
            for way, slot in ends:
                value = value + red_recv[j, way, slot, which].astype(jnp.float32)
            return value.astype(jnp.bfloat16)

        moe_send[j] = moe(their_rows, 1 - c)
        give_rows(j).start()
        value = after_mix[:, cols(c, j)].astype(jnp.float32) + moe(own_rows, c).astype(jnp.float32)
        out[:, cols(c, j)] = value.astype(jnp.bfloat16)

    def take_rows(j):
        give_rows(j).wait_recv()
        value = after_mix[:, cols(1 - c, j)].astype(jnp.float32) + moe_recv[j].astype(jnp.float32)
        out[:, cols(1 - c, j)] = value.astype(jnp.bfloat16)

    down(0)
    for j in range(1, nc):
        down(j)
        add_halves(j - 1)
    add_halves(nc - 1)
    swap_sd.wait_recv()
    blend_rows(0)
    step(0, 1)
    step(0, 2)
    blend_rows(1)
    step(1, 1)
    step(0, 3)
    step(1, 2)
    blend_rows(2)
    step(2, 1)
    step(0, 4)
    step(1, 3)
    step(2, 2)
    blend_rows(3)
    step(3, 1)
    finish(0)
    step(1, 4)
    step(2, 3)
    step(3, 2)
    finish(1)
    step(2, 4)
    step(3, 3)
    finish(2)
    step(3, 4)
    finish(3)
    for j in range(nc):
        take_rows(j)
    swap_sd.wait_send()
    for j in range(nc):
        give(j).wait_send()
        spread.drain(j)
        give_rows(j).wait_send()
        for way in range(2):
            for m in range(1, p.steps(j)[way] + 1):
                red(j, way, m).wait_send()


def vmem():
    return pl.BlockSpec(memory_space=pltpu.VMEM)


def anywhere():
    return pl.BlockSpec(memory_space=pl.ANY)


def dispatch(normed, pick, w_gate, w_up, shared_gate, shared_up):
    nc = CHUNKS
    slots, rows = pick.shape
    width = normed.shape[1]
    half = width // 2
    fc = half // nc
    hidden_units, units = w_gate.shape[0], shared_gate.shape[0]
    hops = lax.axis_size("tp") // 4
    bf, f32 = jnp.bfloat16, jnp.float32
    dma = pltpu.SemaphoreType.DMA
    return pl.pallas_call(
        dispatch_kernel,
        name="dispatch",
        out_shape=(
            jax.ShapeDtypeStruct((slots, hidden_units), bf),
            jax.ShapeDtypeStruct((rows, 2 * units), bf),
        ),
        in_specs=[vmem(), vmem(), anywhere(), anywhere(), vmem(), vmem()],
        out_specs=(vmem(), vmem()),
        scratch_shapes=[
            pltpu.VMEM((nc, rows, fc), bf),
            pltpu.VMEM((nc, slots, fc), bf),
            pltpu.VMEM((nc, slots, fc), bf),
            pltpu.VMEM((nc, slots, fc), bf),
            pltpu.VMEM((hidden_units, width), bf),
            pltpu.VMEM((hidden_units, width), bf),
            pltpu.VMEM((slots, hidden_units), f32),
            pltpu.VMEM((slots, hidden_units), f32),
            pltpu.VMEM((4 * units, half), bf),
            pltpu.VMEM((rows, 4 * units), f32),
            pltpu.VMEM((rows, 4 * units), f32),
            dma((2,)),
            dma((nc,)),
            dma((nc,)),
            dma((nc, 2, hops)),
            dma((nc, 2, hops)),
            dma((nc,)),
            dma((nc,)),
            dma((nc,)),
            dma((nc,)),
            dma((3,)),
            dma((3,)),
        ],
        compiler_params=pltpu.CompilerParams(collective_id=1, has_side_effects=True),
    )(normed, pick, w_gate, w_up, shared_gate, shared_up)


def combine(hidden, w_down, blend, shared, shared_down, after_mix):
    nc = CHUNKS
    rows, slots = blend.shape
    my_rows, width = after_mix.shape
    half = width // 2
    fc = half // nc
    hidden_units, units = w_down.shape[0], shared_down.shape[0]
    hops = lax.axis_size("tp") // 4
    bf, f32 = jnp.bfloat16, jnp.float32
    dma = pltpu.SemaphoreType.DMA
    return pl.pallas_call(
        combine_kernel,
        name="combine",
        out_shape=jax.ShapeDtypeStruct((my_rows, width), bf),
        in_specs=[vmem(), anywhere(), vmem(), vmem(), vmem(), vmem()],
        out_specs=vmem(),
        scratch_shapes=[
            pltpu.VMEM((hidden_units, width), bf),
            pltpu.VMEM((nc, slots, fc), bf),
            pltpu.VMEM((nc, slots, fc), bf),
            pltpu.VMEM((nc, slots, fc), bf),
            pltpu.VMEM((nc, slots, fc), bf),
            pltpu.VMEM((2 * units, half), bf),
            pltpu.VMEM((nc, rows, fc), f32),
            pltpu.VMEM((nc, 2, hops, 2 * my_rows, fc), bf),
            pltpu.VMEM((nc, 2, hops, 2 * my_rows, fc), bf),
            pltpu.VMEM((nc, my_rows, fc), bf),
            pltpu.VMEM((nc, my_rows, fc), bf),
            dma((1,)),
            dma((1,)),
            dma((1,)),
            dma((nc,)),
            dma((nc,)),
            dma((nc,)),
            dma((nc,)),
            dma((nc, 2, hops)),
            dma((nc, 2, hops)),
            dma((nc,)),
            dma((nc,)),
        ],
        compiler_params=pltpu.CompilerParams(collective_id=2, has_side_effects=True),
    )(hidden, w_down, blend, shared, shared_down, after_mix)


def slot_matrices(ids, weights, experts, capacity, lanes, lane):
    rows = ids.shape[0]
    slots = experts // lanes * capacity
    named = ids[:, :, None] == jnp.arange(experts, dtype=jnp.int32)
    weight = jnp.sum(jnp.where(named, weights[:, :, None], 0.0), axis=1)
    named = jnp.any(named, axis=1)
    index = jnp.arange(rows, dtype=jnp.int32)
    before = (index[None, :] < index[:, None]).astype(jnp.bfloat16)
    rank = dot_nn(before, named.astype(jnp.bfloat16))
    rank = jnp.where(named, rank, -1.0).astype(jnp.bfloat16)
    slot = jnp.arange(slots, dtype=jnp.int32)
    holds = slot[:, None] // capacity * lanes + lane == jnp.arange(experts, dtype=jnp.int32)
    holds = holds.astype(jnp.bfloat16)
    place = (slot % capacity).astype(jnp.float32)
    pick = (dot_nt(holds, rank) == place[:, None]).astype(jnp.bfloat16)
    blend = jnp.where(
        dot_nt(rank, holds) == place[None, :], dot_nt(weight.astype(jnp.bfloat16), holds), 0.0
    )
    return pick, blend.astype(jnp.bfloat16)


def body(
    queries,
    keys,
    values,
    sink_logits,
    w_out,
    residual,
    norm_gain,
    expert_ids,
    expert_weights,
    w_gate,
    w_up,
    w_down,
    shared_gate,
    shared_up,
    shared_down,
):
    tp_count = lax.axis_size("tp")
    sp_count = lax.axis_size("sp")
    seq_rows = queries.shape[0]
    expert_count = sp_count * tp_count // 2
    capacity = CAP
    local_heads = queries.shape[1] // HD
    kv_start = lax.axis_index("tp") * local_heads // GROUP * HD
    key_cols = lax.dynamic_slice_in_dim(keys, kv_start, HD, 1)
    value_cols = lax.dynamic_slice_in_dim(values, kv_start, HD, 1)
    rim_keys, rim_values = shifted(
        (key_cols[seq_rows - WINDOW :], value_cols[seq_rows - WINDOW :]), "sp", 1
    )
    num_blocks = seq_rows // WINDOW
    key_blocks = key_cols.reshape(num_blocks, WINDOW, HD)
    value_blocks = value_cols.reshape(num_blocks, WINDOW, HD)
    keys_ext = jnp.concatenate(
        [jnp.concatenate([rim_keys[None], key_blocks[:-1]], axis=0), key_blocks], axis=1
    )
    values_ext = jnp.concatenate(
        [jnp.concatenate([rim_values[None], value_blocks[:-1]], axis=0), value_blocks], axis=1
    )
    query_blocks = queries.reshape(num_blocks, WINDOW, local_heads, HD)
    scores = jnp.einsum(
        "nqhd,nsd->nhqs", query_blocks, keys_ext, preferred_element_type=jnp.float32
    ) * HD ** (-0.5)
    query_pos = jnp.arange(WINDOW)[:, None] + WINDOW
    key_pos = jnp.arange(2 * WINDOW)[None, :]
    in_band = (key_pos <= query_pos) & (key_pos > query_pos - WINDOW)
    absolute = (
        lax.axis_index("sp") * seq_rows
        + jnp.arange(num_blocks)[:, None, None] * WINDOW
        + key_pos[None]
        - WINDOW
    )
    allowed = in_band[None] & (absolute >= 0)
    scores = jnp.where(allowed[:, None], scores, -jnp.inf)
    sink_col = jnp.broadcast_to(sink_logits[None, :, None, None], scores.shape[:-1] + (1,))
    combined = jnp.concatenate([scores, sink_col], axis=-1)
    row_max = jnp.max(combined, axis=-1, keepdims=True)
    exps = jnp.exp(combined - row_max)
    weights = (exps[..., :-1] / jnp.sum(exps, axis=-1, keepdims=True)).astype(jnp.bfloat16)
    attended = jnp.einsum("nhqs,nsd->nqhd", weights, values_ext, preferred_element_type=jnp.float32)
    attended = attended.astype(jnp.bfloat16).reshape(seq_rows, local_heads * HD)
    head_rows = lax.all_to_all(attended, "tp", split_axis=0, concat_axis=1, tiled=True)
    projected = jnp.dot(
        head_rows,
        lax.all_gather(w_out, "tp", axis=0, tiled=True),
        preferred_element_type=jnp.float32,
    )
    after_mix = (residual.astype(jnp.float32) + projected).astype(jnp.bfloat16)
    normed = normalize(after_mix, norm_gain)
    lanes = tp_count // 2
    pick, blend = slot_matrices(
        expert_ids, expert_weights, expert_count, capacity, lanes, lax.axis_index("tp") // 2
    )
    hidden, shared = dispatch(normed, pick, w_gate[0], w_up[0], shared_gate, shared_up)
    return combine(hidden, w_down[0], blend, shared, shared_down, after_mix)


def solution(mesh):
    return jax.shard_map(
        body,
        mesh=mesh,
        in_specs=(
            P("sp", "tp"),
            P("sp", None),
            P("sp", None),
            P("tp"),
            P("tp", None),
            P(("sp", "tp"), None),
            P(),
            P("sp", None),
            P("sp", None),
            P(("sp", "tp"), None, None),
            P(("sp", "tp"), None, None),
            P(("sp", "tp"), None, None),
            P("tp", None),
            P("tp", None),
            P("tp", None),
        ),
        out_specs=P(("sp", "tp"), None),
        check_vma=False,
    )
```

```python
import jax
import jax.numpy as jnp
from jax import lax
from jax.experimental import pallas as pl
from jax.experimental.pallas import tpu as pltpu
from jax.sharding import PartitionSpec as P

HD = 64
GROUP = 4
WINDOW = 128
TOPK = 4


MESH = pl.DeviceIdType.MESH
CHUNKS = 4
CAP = 64


def dot_nt(a, b):
    return lax.dot_general(a, b, (((1,), (1,)), ((), ())), preferred_element_type=jnp.float32)


def dot_nn(a, b):
    return jnp.dot(a, b, preferred_element_type=jnp.float32)


def rows_loop(total, step, fn):
    def one(i, carry):
        fn(pl.ds(pl.multiple_of(i * step, step), step))
        return carry

    lax.fori_loop(0, total // step, one, 0)


class Place:
    def __init__(self):
        self.sp_count = lax.axis_size("sp")
        self.tp_count = lax.axis_size("tp")
        self.s = lax.axis_index("sp")
        self.t = lax.axis_index("tp")
        self.c = self.t % 2
        self.z = self.t // 2
        self.nz = self.tp_count // 2
        self.partner = (self.s, self.t + 1 - 2 * self.c)
        self.right = (self.s, (self.t + 2) % self.tp_count)
        self.left = (self.s, (self.t + self.tp_count - 2) % self.tp_count)

    def peer(self, o):
        return ((self.s + o) % self.sp_count, self.t)

    def barrier(self, devices, peers=True):
        sem = pltpu.get_barrier_semaphore()
        for device in devices:
            pl.semaphore_signal(sem, inc=1, device_id=device, device_id_type=MESH)
        count = len(devices)
        if peers:

            def one(o, carry):
                pl.semaphore_signal(sem, inc=1, device_id=self.peer(o), device_id_type=MESH)
                return carry

            lax.fori_loop(1, self.sp_count, one, 0)
            count += self.sp_count - 1
        pl.semaphore_wait(sem, count)

    def steps(self, j):
        far, near = self.nz // 2, self.nz - 1 - self.nz // 2
        return (far, near) if j % 2 == 0 else (near, far)


def remote(src, dst, send_sem, recv_sem, device):
    return pltpu.make_async_remote_copy(
        src_ref=src, dst_ref=dst, send_sem=send_sem, recv_sem=recv_sem, device_id=device, device_id_type=MESH
    )


class RingGather:
    def __init__(self, p, buf, rows, send_sems, recv_sems):
        self.p, self.buf, self.rows = p, buf, rows
        self.ss, self.rs = send_sems, recv_sems

    def copy(self, j, way, k, shift):
        p = self.p
        origin = (p.z - shift if way == 0 else p.z + shift) + p.nz
        block = self.buf.at[j, pl.ds(pl.multiple_of(origin % p.nz * self.rows, self.rows), self.rows)]
        return remote(block, block, self.ss.at[j, way, k - 1], self.rs.at[j, way, k - 1], p.left if way else p.right)

    def send(self, j, k):
        for way in range(2):
            if k <= self.p.steps(j)[way]:
                self.copy(j, way, k, k - 1).start()

    def wait(self, j, k):
        for way in range(2):
            if k <= self.p.steps(j)[way]:
                self.copy(j, way, k, k).wait_recv()

    def drain(self, j):
        for way in range(2):
            for k in range(1, self.p.steps(j)[way] + 1):
                self.copy(j, way, k, k - 1).wait_send()


class Exchange:
    def __init__(self, p, src, dst, rows, send_sems, recv_sems):
        self.p, self.src, self.dst, self.rows = p, src, dst, rows
        self.ss, self.rs = send_sems, recv_sems

    def block(self, index):
        return pl.ds(pl.multiple_of(index * self.rows, self.rows), self.rows)

    def send(self, j):
        p = self.p

        def one(o, carry):
            peer = p.peer(o)
            remote(
                self.src.at[j, self.block(peer[0])],
                self.dst.at[j, self.block(p.s)],
                self.ss.at[j],
                self.rs.at[j],
                peer,
            ).start()
            return carry

        lax.fori_loop(1, p.sp_count, one, 0)
        self.dst[j, self.block(p.s)] = self.src[j, self.block(p.s)]

    def all_of(self, j):
        others = pl.ds(0, (self.p.sp_count - 1) * self.rows)
        return remote(self.src.at[j, others], self.dst.at[j, others], self.ss.at[j], self.rs.at[j], self.p.peer(1))

    def wait(self, j):
        self.all_of(j).wait_recv()

    def drain(self, j):
        self.all_of(j).wait_send()


def mix_kernel(
    queries, keys, values, sink, w_out, residual, gain, ids, weights,
    normed, after, pick, blend,
    key_ext, value_ext, att, heads, heads_t, wide, res, square, square_other,
    rank_buf, weight_buf,
    k_send, k_recv, h_send, h_recv, x_send, x_recv, ring_send, ring_recv, r_send, r_recv, q_send, q_recv,
):
    p = Place()
    c, nc = p.c, CHUNKS
    rows = queries.shape[0]
    my_rows, width = residual.shape
    half = width // 2
    fc = half // nc
    head_rows = w_out.shape[0]
    chip_rows = 2 * my_rows
    blocks = rows // WINDOW
    experts = p.sp_count * p.nz
    kv = p.t // GROUP
    kv_cols = pl.ds(pl.multiple_of(kv // 2 * 128, 128), 128)
    f32, bf = jnp.float32, jnp.bfloat16

    sem = pltpu.get_barrier_semaphore()

    def greet(o, carry):
        pl.semaphore_signal(
            sem, inc=1, device_id=(p.s, (p.t + o) % p.tp_count), device_id_type=MESH
        )
        return carry

    lax.fori_loop(1, p.tp_count, greet, 0)
    following = ((p.s + 1) % p.sp_count, p.t)
    for device in (following, ((p.s + p.sp_count - 1) % p.sp_count, p.t)):
        pl.semaphore_signal(sem, inc=1, device_id=device, device_id_type=MESH)
    pl.semaphore_wait(sem, p.tp_count + 1)

    rim = pl.ds(rows - WINDOW, WINDOW)
    halo = [
        remote(ref.at[rim, kv_cols], ext.at[pl.ds(0, WINDOW)], k_send.at[i], k_recv.at[i], following)
        for i, (ref, ext) in enumerate(((keys, key_ext), (values, value_ext)))
    ]

    def half_of(h):
        return pl.ds(pl.multiple_of(h * half, half), half)

    def cols(h, j):
        return pl.ds(pl.multiple_of(h * half + j * fc, fc), fc)

    def shard(core):
        return pl.ds(pl.multiple_of(p.z * 2 * head_rows + core * head_rows, head_rows), head_rows)

    def swap(j, core):
        return remote(
            w_out.at[:, cols(1 - c, j)], wide.at[j, shard(core)], x_send.at[j], x_recv.at[j], p.partner
        )

    my_part = pl.ds(pl.multiple_of(c * my_rows, my_rows), my_rows)
    swap_res = remote(residual.at[:, half_of(1 - c)], res.at[my_part], r_send.at[0], r_recv.at[0], p.partner)
    for j in range(nc):
        swap(j, c).start()
    sends_rim, gets_rim = p.s + 1 < p.sp_count, p.s > 0

    @pl.when(sends_rim)
    def _():
        for copy in halo:
            copy.start()

    swap_res.start()
    for j in range(nc):
        wide[j, shard(c)] = w_out[:, cols(c, j)]
    res[my_part] = residual[:, half_of(c)]
    ring = RingGather(p, wide, 2 * head_rows, ring_send, ring_recv)
    last = p.nz // 2
    everything = tuple(range(nc))
    for j in everything:
        swap(j, 1 - c).wait_recv()
        ring.send(j, 1)

    def hop(k):
        for j in everything:
            ring.wait(j, k)
            ring.send(j, k + 1)

    key_ext[pl.ds(WINDOW, rows)] = keys[:, kv_cols]
    value_ext[pl.ds(WINDOW, rows)] = values[:, kv_cols]

    @pl.when(jnp.logical_not(gets_rim))
    def _():
        key_ext[pl.ds(0, WINDOW)] = jnp.zeros((WINDOW, 128), bf)
        value_ext[pl.ds(0, WINDOW)] = jnp.zeros((WINDOW, 128), bf)

    tile = min(256, rows)
    capacity = pick.shape[0] // p.sp_count
    slots = pick.shape[0]
    shift = capacity.bit_length() - 1

    def iota(shape, axis):
        return lax.broadcasted_iota(jnp.int32, shape, axis)

    def name_rows(r):
        lanes = iota((tile, experts), 1)
        named = jnp.zeros((tile, experts), f32)
        weight = jnp.zeros((tile, experts), f32)
        tile_ids, tile_weights = ids[r], weights[r]
        for k in range(TOPK):
            same = tile_ids[:, k : k + 1] == lanes
            named = jnp.where(same, 1.0, named)
            weight = jnp.where(same, tile_weights[:, k : k + 1], weight)
        rank_buf[r] = named.astype(bf)
        weight_buf[r] = weight.astype(bf)

    rows_loop(rows, tile, name_rows)
    all_named = rank_buf[...]
    ranks = []
    for i in range(rows // tile):
        before = iota((tile, rows), 1) < iota((tile, rows), 0) + i * tile
        rank = dot_nn(jnp.where(before, 1.0, 0.0).astype(bf), all_named)
        named = all_named[i * tile : (i + 1) * tile].astype(f32) > 0.0
        ranks.append(jnp.where(named, rank, -1.0).astype(bf))
    for i, rank in enumerate(ranks):
        rank_buf[pl.ds(i * tile, tile)] = rank

    def holds(first, count):
        slot = iota((count, experts), 0) + first
        same = jnp.right_shift(slot, shift) * p.nz + p.z == iota((count, experts), 1)
        return jnp.where(same, 1.0, 0.0).astype(bf)

    def fill_pick(i, carry):
        first = i * tile
        place = jnp.bitwise_and(iota((tile, rows), 0) + first, capacity - 1).astype(f32)
        hit = dot_nt(holds(first, tile), rank_buf[...]) == place
        pick[pl.ds(pl.multiple_of(first, tile), tile)] = jnp.where(hit, 1.0, 0.0).astype(bf)
        return carry

    lax.fori_loop(0, slots // tile, fill_pick, 0)
    all_holds = holds(0, slots)

    def fill_blend(r):
        place = jnp.bitwise_and(iota((tile, slots), 1), capacity - 1).astype(f32)
        hit = dot_nt(rank_buf[r], all_holds) == place
        blend[r] = jnp.where(hit, dot_nt(weight_buf[r], all_holds), 0.0).astype(bf)

    @pl.when(gets_rim)
    def _():
        for copy in halo:
            copy.wait_recv()

    lane_half = kv % 2
    sink_value = sink[...]

    def attend(i, carry):
        b = (p.z + i) % blocks
        ext = pl.ds(pl.multiple_of(b * WINDOW, WINDOW), 2 * WINDOW)
        query = queries[pl.ds(pl.multiple_of(b * WINDOW, WINDOW), WINDOW)]
        query = jnp.concatenate([query, query], axis=1)
        in_half = jnp.right_shift(iota((WINDOW, 2 * HD), 1), HD.bit_length() - 1) == lane_half
        query = jnp.where(in_half, query.astype(f32), 0.0).astype(bf)
        scores = dot_nt(key_ext[ext], query) * HD ** (-0.5)
        key_pos = iota((2 * WINDOW, WINDOW), 0)
        query_pos = iota((2 * WINDOW, WINDOW), 1) + WINDOW
        first_key = jnp.where(p.s * blocks + b == 0, WINDOW, 0)
        allowed = (key_pos <= query_pos) & (key_pos > query_pos - WINDOW) & (key_pos >= first_key)
        scores = jnp.where(allowed, scores, -jnp.inf)
        top = jnp.maximum(jnp.max(scores, axis=0, keepdims=True), sink_value)
        exps = jnp.exp(scores - top)
        total = jnp.sum(exps, axis=0, keepdims=True) + jnp.exp(sink_value - top)
        shares = (exps / total).astype(bf)
        both = lax.dot_general(
            value_ext[ext], shares, (((0,), (0,)), ((), ())), preferred_element_type=f32
        )
        att[b] = jnp.where(lane_half == 0, both[:HD], both[HD:]).astype(bf)
        for core in range(2):
            target = 2 * b + core

            @pl.when(target != p.t)
            def _():
                head_piece(b, (p.s, target)).start()

            @pl.when(target == p.t)
            def _():
                heads[head_place] = att[b]

        return carry

    head_place = pl.ds(pl.multiple_of(p.t * HD, HD), HD)

    def head_piece(b, device):
        return remote(att.at[b], heads.at[head_place], h_send.at[0], h_recv.at[0], device)

    others = heads.at[pl.ds(0, (p.tp_count - 1) * HD)]
    head_total = remote(others, others, h_send.at[0], h_recv.at[0], p.partner)

    lax.fori_loop(0, blocks // 2, attend, 0)
    for k in range(1, last):
        hop(k)
        if k == 1:
            lax.fori_loop(blocks // 2, blocks, attend, 0)
        if k == min(2, last - 1):
            rows_loop(rows, tile, fill_blend)
    head_total.wait_recv()
    heads_t[...] = heads[...].T
    swap_res_in = remote(
        residual.at[:, half_of(1 - c)],
        res.at[pl.ds(pl.multiple_of((1 - c) * my_rows, my_rows), my_rows)],
        r_send.at[0], r_recv.at[0], p.partner,
    )
    swap_res_in.wait_recv()
    squares = jnp.zeros((chip_rows, 1), f32)
    for j in range(nc):
        ring.wait(j, last)
        piece = pl.ds(j * fc, fc)
        mixed = res[:, piece].astype(f32) + dot_nn(heads_t[...], wide[j])
        mixed = mixed.astype(bf)
        after[:, piece] = mixed
        mixed = mixed.astype(f32)
        squares = squares + jnp.sum(mixed * mixed, axis=1, keepdims=True)
    square[...] = jnp.broadcast_to(squares, square.shape)
    swap_square = remote(square, square_other, q_send.at[0], q_recv.at[0], p.partner)
    swap_square.start()
    swap_square.wait_recv()
    mean = (square[...] + square_other[...])[:, :1] / width
    scale = lax.rsqrt(mean + 1e-06)
    for j in range(nc):
        piece = pl.ds(j * fc, fc)
        normed[:, piece] = (after[:, piece].astype(f32) * scale * gain[:, cols(c, j)]).astype(bf)

    @pl.when(sends_rim)
    def _():
        for copy in halo:
            copy.wait_send()

    for j in range(nc):
        swap(j, c).wait_send()
        ring.drain(j)
    swap_res.wait_send()
    head_total.wait_send()
    swap_square.wait_send()


def dispatch_kernel(
    normed, pick, wg_hbm, wu_hbm, sg, su, hidden, shared,
    ring_buf, outgoing, own, other, wg, wu, gate_sum, up_sum, sgu, pre, pre_other,
    w_sem, ring_send, ring_recv, a_send, a_recv, f_send, f_recv, s_send, s_recv,
):
    p = Place()
    c, nc = p.c, CHUNKS
    slots, rows = pick.shape
    chip_rows, half = normed.shape
    fc = half // nc
    units = sg.shape[0]
    tile = min(256, slots)
    fetch_gate = pltpu.make_async_copy(wg_hbm, wg, w_sem.at[0])
    fetch_up = pltpu.make_async_copy(wu_hbm, wu, w_sem.at[1])
    fetch_gate.start()
    fetch_up.start()
    p.barrier([p.partner, p.right, p.left])

    mine = pl.ds(pl.multiple_of(p.z * chip_rows, chip_rows), chip_rows)

    def cols(h, j):
        return pl.ds(pl.multiple_of(h * half + j * fc, fc), fc)

    half_cols = [pl.ds(pl.multiple_of(h * half, half), half) for h in (c, 1 - c)]
    sgu_rows = [pl.ds(pl.multiple_of(k * 2 * units + c * units, units), units) for k in range(2)]
    shared_swaps = [
        remote(ref.at[:, half_cols[1]], sgu.at[sgu_rows[k]], s_send.at[k], s_recv.at[k], p.partner)
        for k, ref in enumerate((sg, su))
    ]
    for copy in shared_swaps:
        copy.start()
    for k, ref in enumerate((sg, su)):
        sgu[sgu_rows[k]] = ref[:, half_cols[0]]
    for j in range(nc):
        ring_buf[j, mine] = normed[:, j * fc : (j + 1) * fc]

    ring = RingGather(p, ring_buf, chip_rows, ring_send, ring_recv)
    spread = Exchange(p, outgoing, own, slots // p.sp_count, a_send, a_recv)
    last = p.nz // 2

    def forward(j):
        return remote(own.at[j], other.at[j], f_send.at[j], f_recv.at[j], p.partner)

    def begin(pair):
        for j in pair:
            ring.send(j, 1)

    def hop(pair, k):
        for j in pair:
            ring.wait(j, k)
            ring.send(j, k + 1)

    def select(j):
        ring.wait(j, last)

        def one(r):
            outgoing[j, r] = dot_nn(pick[r], ring_buf[j]).astype(jnp.bfloat16)

        rows_loop(slots, tile, one)
        spread.send(j)

    def shared_part(j):
        def one(r):
            part = dot_nt(ring_buf[j, r], sgu[:, j * fc : (j + 1) * fc])
            pre[r] = part if j == 0 else pre[r] + part

        rows_loop(rows, tile, one)

    def arrive(j):
        spread.wait(j)
        forward(j).start()

    def multiply(j):
        forward(j).wait_recv()

        def one(r):
            a, b = own[j, r], other[j, r]
            for w, total in ((wg, gate_sum), (wu, up_sum)):
                part = dot_nt(a, w[:, cols(c, j)]) + dot_nt(b, w[:, cols(1 - c, j)])
                total[r] = part if j == 0 else total[r] + part

        rows_loop(slots, tile, one)

    first, second = (0, 1), (2, 3)
    begin(first)
    for k in range(1, last):
        hop(first, k)
    begin(second)
    for j in first:
        select(j)
    for copy in shared_swaps:
        copy.wait_recv()
    for k in range(1, last):
        hop(second, k)
        if k <= 2:
            shared_part(first[k - 1])
    for j in first:
        if last <= j + 1:
            shared_part(j)
    select(2)
    arrive(0)
    select(3)
    for j in second:
        shared_part(j)
    swap_pre = remote(pre, pre_other, s_send.at[2], s_recv.at[2], p.partner)
    swap_pre.start()
    fetch_gate.wait()
    fetch_up.wait()
    multiply(0)
    arrive(1)
    swap_pre.wait_recv()

    def shared_one(r):
        both = pre[r] + pre_other[r]
        gate, up = both[:, : 2 * units], both[:, 2 * units :]
        shared[r] = (gate / (1.0 + jnp.exp(-gate)) * up).astype(jnp.bfloat16)

    rows_loop(rows, tile, shared_one)
    multiply(1)
    arrive(2)
    multiply(2)
    arrive(3)
    multiply(3)

    def hidden_one(r):
        gate = gate_sum[r]
        hidden[r] = (gate / (1.0 + jnp.exp(-gate)) * up_sum[r]).astype(jnp.bfloat16)

    rows_loop(slots, tile, hidden_one)
    for j in range(nc):
        ring.drain(j)
        spread.drain(j)
        forward(j).wait_send()
    for copy in shared_swaps:
        copy.wait_send()
    swap_pre.wait_send()


def combine_kernel(
    hidden, wd_hbm, blend, shared, sd, after_mix, out,
    wd, half_send, half_recv, total, held, sdh, part, red_send, red_recv, moe_send, moe_recv,
    w_sem, d_send, d_recv, h_send, h_recv, a_send, a_recv, r_send, r_recv, m_send, m_recv,
):
    p = Place()
    c, nc = p.c, CHUNKS
    rows, slots = blend.shape
    chip_rows, half = after_mix.shape
    my_rows = chip_rows // 2
    fc = half // nc
    units = sd.shape[0]
    tile = min(256, slots)
    fetch = pltpu.make_async_copy(wd_hbm, wd, w_sem.at[0])
    fetch.start()
    p.barrier([p.partner, p.right, p.left])

    def cols(h, j):
        return pl.ds(pl.multiple_of(h * half + j * fc, fc), fc)

    half_cols = [pl.ds(pl.multiple_of(h * half, half), half) for h in (c, 1 - c)]
    my_units = pl.ds(pl.multiple_of(c * units, units), units)
    swap_sd = remote(sd.at[:, half_cols[1]], sdh.at[my_units], d_send.at[0], d_recv.at[0], p.partner)
    swap_sd.start()
    sdh[my_units] = sd[:, half_cols[0]]
    fetch.wait()

    spread = Exchange(p, total, held, slots // p.sp_count, a_send, a_recv)

    def give(j):
        return remote(half_send.at[j], half_recv.at[j], h_send.at[j], h_recv.at[j], p.partner)

    def down(j):
        def theirs(r):
            half_send[j, r] = dot_nn(hidden[r], wd[:, cols(1 - c, j)]).astype(jnp.bfloat16)

        def ours(r):
            total[j, r] = dot_nn(hidden[r], wd[:, cols(c, j)]).astype(jnp.bfloat16)

        rows_loop(slots, tile, theirs)
        give(j).start()
        rows_loop(slots, tile, ours)

    def add_halves(j):
        give(j).wait_recv()

        def one(r):
            both = total[j, r].astype(jnp.float32) + half_recv[j, r].astype(jnp.float32)
            total[j, r] = both.astype(jnp.bfloat16)

        rows_loop(slots, tile, one)
        spread.send(j)

    def blend_rows(j):
        spread.wait(j)

        def one(r):
            mixed = dot_nn(blend[r], held[j])
            part[j, r] = mixed + dot_nn(shared[r], sdh[:, j * fc : (j + 1) * fc])

        rows_loop(rows, tile, one)

    def chip_block(distance):
        index = (p.z + distance + p.nz) % p.nz
        return pl.ds(pl.multiple_of(index * chip_rows, chip_rows), chip_rows)

    def red(j, way, m):
        return remote(
            red_send.at[j, way, m - 1],
            red_recv.at[j, way, m - 1],
            r_send.at[j, way, m - 1],
            r_recv.at[j, way, m - 1],
            p.left if way else p.right,
        )

    def step(j, m):
        for way in range(2):
            n = p.steps(j)[way]
            if m > n:
                continue
            distance = n - m + 1
            value = part[j, chip_block(-distance if way else distance)]
            if m > 1:
                red(j, way, m - 1).wait_recv()
                value = value + red_recv[j, way, m - 2].astype(jnp.float32)
            red_send[j, way, m - 1] = value.astype(jnp.bfloat16)
            red(j, way, m).start()

    def give_rows(j):
        return remote(moe_send.at[j], moe_recv.at[j], m_send.at[j], m_recv.at[j], p.partner)

    def finish(j):
        own_rows = pl.ds(pl.multiple_of(c * my_rows, my_rows), my_rows)
        their_rows = pl.ds(pl.multiple_of((1 - c) * my_rows, my_rows), my_rows)
        ends = []
        for way in range(2):
            n = p.steps(j)[way]
            if n:
                red(j, way, n).wait_recv()
                ends.append((way, n - 1))

        def layer_rows(which, offset):
            base = pl.ds(pl.multiple_of(p.z * chip_rows + offset * my_rows, my_rows), my_rows)
            value = part[j, base]
            for way, slot in ends:
                value = value + red_recv[j, way, slot, which].astype(jnp.float32)
            moe = value.astype(jnp.bfloat16).astype(jnp.float32)
            before = after_mix[which, j * fc : (j + 1) * fc].astype(jnp.float32)
            return (before + moe).astype(jnp.bfloat16)

        moe_send[j] = layer_rows(their_rows, 1 - c)
        give_rows(j).start()
        out[:, cols(c, j)] = layer_rows(own_rows, c)

    def take_rows(j):
        give_rows(j).wait_recv()
        out[:, cols(1 - c, j)] = moe_recv[j]

    down(0)
    for j in range(1, nc):
        down(j)
        add_halves(j - 1)
    add_halves(nc - 1)
    swap_sd.wait_recv()
    blend_rows(0)
    step(0, 1)
    step(0, 2)
    blend_rows(1)
    step(1, 1)
    step(0, 3)
    step(1, 2)
    blend_rows(2)
    step(2, 1)
    step(0, 4)
    step(1, 3)
    step(2, 2)
    blend_rows(3)
    step(3, 1)
    finish(0)
    step(1, 4)
    step(2, 3)
    step(3, 2)
    finish(1)
    step(2, 4)
    step(3, 3)
    finish(2)
    step(3, 4)
    finish(3)
    for j in range(nc):
        take_rows(j)
    swap_sd.wait_send()
    for j in range(nc):
        give(j).wait_send()
        spread.drain(j)
        give_rows(j).wait_send()
        for way in range(2):
            for m in range(1, p.steps(j)[way] + 1):
                red(j, way, m).wait_send()


def vmem():
    return pl.BlockSpec(memory_space=pltpu.VMEM)


def anywhere():
    return pl.BlockSpec(memory_space=pl.ANY)


def mix(queries, keys, values, sink, w_out, residual, gain, ids, weights, capacity):
    nc = CHUNKS
    rows = queries.shape[0]
    my_rows, width = residual.shape
    half = width // 2
    fc = half // nc
    tp_count, sp_count = lax.axis_size("tp"), lax.axis_size("sp")
    experts = sp_count * tp_count // 2
    slots = sp_count * capacity
    hops = tp_count // 4
    bf, f32 = jnp.bfloat16, jnp.float32
    dma = pltpu.SemaphoreType.DMA
    return pl.pallas_call(
        mix_kernel,
        name="mix",
        out_shape=(
            jax.ShapeDtypeStruct((2 * my_rows, half), bf),
            jax.ShapeDtypeStruct((2 * my_rows, half), bf),
            jax.ShapeDtypeStruct((slots, rows), bf),
            jax.ShapeDtypeStruct((rows, slots), bf),
        ),
        in_specs=[vmem()] * 9,
        out_specs=(vmem(),) * 4,
        scratch_shapes=[
            pltpu.VMEM((rows + WINDOW, 128), bf),
            pltpu.VMEM((rows + WINDOW, 128), bf),
            pltpu.VMEM((rows // WINDOW, HD, WINDOW), bf),
            pltpu.VMEM((tp_count * HD, 2 * my_rows), bf),
            pltpu.VMEM((2 * my_rows, tp_count * HD), bf),
            pltpu.VMEM((nc, tp_count * HD, fc), bf),
            pltpu.VMEM((2 * my_rows, half), bf),
            pltpu.VMEM((2 * my_rows, 128), f32),
            pltpu.VMEM((2 * my_rows, 128), f32),
            pltpu.VMEM((rows, experts), bf),
            pltpu.VMEM((rows, experts), bf),
            dma((2,)),
            dma((2,)),
            dma((1,)),
            dma((1,)),
            dma((nc,)),
            dma((nc,)),
            dma((nc, 2, hops)),
            dma((nc, 2, hops)),
            dma((1,)),
            dma((1,)),
            dma((1,)),
            dma((1,)),
        ],
        compiler_params=pltpu.CompilerParams(collective_id=3, has_side_effects=True),
    )(queries, keys, values, sink, w_out, residual, gain, ids, weights)


def dispatch(normed, pick, w_gate, w_up, shared_gate, shared_up):
    nc = CHUNKS
    slots, rows = pick.shape
    half = normed.shape[1]
    width = 2 * half
    fc = half // nc
    hidden_units, units = w_gate.shape[0], shared_gate.shape[0]
    hops = lax.axis_size("tp") // 4
    bf, f32 = jnp.bfloat16, jnp.float32
    dma = pltpu.SemaphoreType.DMA
    return pl.pallas_call(
        dispatch_kernel,
        name="dispatch",
        out_shape=(
            jax.ShapeDtypeStruct((slots, hidden_units), bf),
            jax.ShapeDtypeStruct((rows, 2 * units), bf),
        ),
        in_specs=[vmem(), vmem(), anywhere(), anywhere(), vmem(), vmem()],
        out_specs=(vmem(), vmem()),
        scratch_shapes=[
            pltpu.VMEM((nc, rows, fc), bf),
            pltpu.VMEM((nc, slots, fc), bf),
            pltpu.VMEM((nc, slots, fc), bf),
            pltpu.VMEM((nc, slots, fc), bf),
            pltpu.VMEM((hidden_units, width), bf),
            pltpu.VMEM((hidden_units, width), bf),
            pltpu.VMEM((slots, hidden_units), f32),
            pltpu.VMEM((slots, hidden_units), f32),
            pltpu.VMEM((4 * units, half), bf),
            pltpu.VMEM((rows, 4 * units), f32),
            pltpu.VMEM((rows, 4 * units), f32),
            dma((2,)),
            dma((nc, 2, hops)),
            dma((nc, 2, hops)),
            dma((nc,)),
            dma((nc,)),
            dma((nc,)),
            dma((nc,)),
            dma((3,)),
            dma((3,)),
        ],
        compiler_params=pltpu.CompilerParams(collective_id=1, has_side_effects=True),
    )(normed, pick, w_gate, w_up, shared_gate, shared_up)


def combine(hidden, w_down, blend, shared, shared_down, after_mix):
    nc = CHUNKS
    rows, slots = blend.shape
    my_rows, half = after_mix.shape[0] // 2, after_mix.shape[1]
    width = 2 * half
    fc = half // nc
    hidden_units, units = w_down.shape[0], shared_down.shape[0]
    hops = lax.axis_size("tp") // 4
    bf, f32 = jnp.bfloat16, jnp.float32
    dma = pltpu.SemaphoreType.DMA
    return pl.pallas_call(
        combine_kernel,
        name="combine",
        out_shape=jax.ShapeDtypeStruct((my_rows, width), bf),
        in_specs=[vmem(), anywhere(), vmem(), vmem(), vmem(), vmem()],
        out_specs=vmem(),
        scratch_shapes=[
            pltpu.VMEM((hidden_units, width), bf),
            pltpu.VMEM((nc, slots, fc), bf),
            pltpu.VMEM((nc, slots, fc), bf),
            pltpu.VMEM((nc, slots, fc), bf),
            pltpu.VMEM((nc, slots, fc), bf),
            pltpu.VMEM((2 * units, half), bf),
            pltpu.VMEM((nc, rows, fc), f32),
            pltpu.VMEM((nc, 2, hops, 2 * my_rows, fc), bf),
            pltpu.VMEM((nc, 2, hops, 2 * my_rows, fc), bf),
            pltpu.VMEM((nc, my_rows, fc), bf),
            pltpu.VMEM((nc, my_rows, fc), bf),
            dma((1,)),
            dma((1,)),
            dma((1,)),
            dma((nc,)),
            dma((nc,)),
            dma((nc,)),
            dma((nc,)),
            dma((nc, 2, hops)),
            dma((nc, 2, hops)),
            dma((nc,)),
            dma((nc,)),
        ],
        compiler_params=pltpu.CompilerParams(collective_id=2, has_side_effects=True),
    )(hidden, w_down, blend, shared, shared_down, after_mix)


def body(
    queries,
    keys,
    values,
    sink_logits,
    w_out,
    residual,
    norm_gain,
    expert_ids,
    expert_weights,
    w_gate,
    w_up,
    w_down,
    shared_gate,
    shared_up,
    shared_down,
):
    normed, after_mix, pick, blend = mix(
        queries,
        keys,
        values,
        sink_logits[:, None],
        w_out,
        residual,
        norm_gain[None, :],
        expert_ids,
        expert_weights,
        CAP,
    )
    hidden, shared = dispatch(normed, pick, w_gate[0], w_up[0], shared_gate, shared_up)
    return combine(hidden, w_down[0], blend, shared, shared_down, after_mix)


def solution(mesh):
    return jax.shard_map(
        body,
        mesh=mesh,
        in_specs=(
            P("sp", "tp"),
            P("sp", None),
            P("sp", None),
            P("tp"),
            P("tp", None),
            P(("sp", "tp"), None),
            P(),
            P("sp", None),
            P("sp", None),
            P(("sp", "tp"), None, None),
            P(("sp", "tp"), None, None),
            P(("sp", "tp"), None, None),
            P("tp", None),
            P("tp", None),
            P("tp", None),
        ),
        out_specs=P(("sp", "tp"), None),
        check_vma=False,
    )
```

```python
import jax
import jax.numpy as jnp
from jax import lax
from jax.experimental import pallas as pl
from jax.experimental.pallas import tpu as pltpu
from jax.sharding import PartitionSpec as P

HD = 64
GROUP = 4
WINDOW = 128
TOPK = 4


MESH = pl.DeviceIdType.MESH
CHUNKS = 4
CUTS = (2, 2, 2, 1, 1)
CAP = 64


def dot_nt(a, b):
    return lax.dot_general(a, b, (((1,), (1,)), ((), ())), preferred_element_type=jnp.float32)


def dot_nn(a, b):
    return jnp.dot(a, b, preferred_element_type=jnp.float32)


def rows_loop(total, step, fn):
    def one(i, carry):
        fn(pl.ds(pl.multiple_of(i * step, step), step))
        return carry

    lax.fori_loop(0, total // step, one, 0)


class Place:
    def __init__(self):
        self.sp_count = lax.axis_size("sp")
        self.tp_count = lax.axis_size("tp")
        self.s = lax.axis_index("sp")
        self.t = lax.axis_index("tp")
        self.c = self.t % 2
        self.z = self.t // 2
        self.nz = self.tp_count // 2
        self.partner = (self.s, self.t + 1 - 2 * self.c)
        self.right = (self.s, (self.t + 2) % self.tp_count)
        self.left = (self.s, (self.t + self.tp_count - 2) % self.tp_count)

    def peer(self, o):
        return ((self.s + o) % self.sp_count, self.t)

    def barrier(self):
        sem = pltpu.get_barrier_semaphore()

        def greet(count, device):
            def one(o, carry):
                pl.semaphore_signal(sem, inc=1, device_id=device(o), device_id_type=MESH)
                return carry

            lax.fori_loop(1, count, one, 0)

        greet(self.tp_count, lambda o: (self.s, (self.t + o) % self.tp_count))
        greet(self.sp_count, self.peer)
        pl.semaphore_wait(sem, self.tp_count + self.sp_count - 2)

    def steps(self, j):
        far, near = self.nz // 2, self.nz - 1 - self.nz // 2
        return (far, near) if j % 2 == 0 else (near, far)


def remote(src, dst, send_sem, recv_sem, device):
    return pltpu.make_async_remote_copy(
        src_ref=src, dst_ref=dst, send_sem=send_sem, recv_sem=recv_sem, device_id=device, device_id_type=MESH
    )


class RingGather:
    def __init__(self, p, buf, rows, send_sems, recv_sems):
        self.p, self.buf, self.rows = p, buf, rows
        self.ss, self.rs = send_sems, recv_sems

    def copy(self, j, way, k, shift):
        p = self.p
        origin = (p.z - shift if way == 0 else p.z + shift) + p.nz
        block = self.buf.at[j, pl.ds(pl.multiple_of(origin % p.nz * self.rows, self.rows), self.rows)]
        return remote(block, block, self.ss.at[j, way, k - 1], self.rs.at[j, way, k - 1], p.left if way else p.right)

    def send(self, j, k):
        for way in range(2):
            if k <= self.p.steps(j)[way]:
                self.copy(j, way, k, k - 1).start()

    def wait(self, j, k):
        for way in range(2):
            if k <= self.p.steps(j)[way]:
                self.copy(j, way, k, k).wait_recv()

    def drain(self, j):
        for way in range(2):
            for k in range(1, self.p.steps(j)[way] + 1):
                self.copy(j, way, k, k - 1).wait_send()


class Exchange:
    def __init__(self, p, src, dst, rows, spans, send_sems, recv_sems):
        self.p, self.src, self.dst, self.rows, self.spans = p, src, dst, rows, spans
        self.ss, self.rs = send_sems, recv_sems

    def block(self, index, j):
        return pl.ds(pl.multiple_of(index * self.rows, self.rows), self.rows), self.spans[j]

    def send(self, j):
        p = self.p

        def one(o, carry):
            peer = p.peer(o)
            remote(
                self.src.at[self.block(peer[0], j)],
                self.dst.at[self.block(p.s, j)],
                self.ss.at[j],
                self.rs.at[j],
                peer,
            ).start()
            return carry

        lax.fori_loop(1, p.sp_count, one, 0)
        self.dst[self.block(p.s, j)] = self.src[self.block(p.s, j)]

    def all_of(self, j):
        others = pl.ds(0, (self.p.sp_count - 1) * self.rows), self.spans[j]
        return remote(self.src.at[others], self.dst.at[others], self.ss.at[j], self.rs.at[j], self.p.peer(1))

    def wait(self, j):
        self.all_of(j).wait_recv()

    def drain(self, j):
        self.all_of(j).wait_send()


def iota(shape, axis):
    return lax.broadcasted_iota(jnp.int32, shape, axis)


def silu_times(gate, up):
    return (gate / (1.0 + jnp.exp(-gate)) * up).astype(jnp.bfloat16)


def layer_kernel(
    queries, keys, values, sink, w_out, residual, gain, ids, weights, wg_hbm, wu_hbm, wd_hbm, sg, su, sd,
    out,
    key_ext, value_ext, att, heads, heads_t, wide, res, after, square, square_other,
    rank_buf, rank_t, weight_buf, pick, blend, scale_rows, scale_cols, scale_slots,
    ring_buf, outgoing, own, other, wg, wu, gate_sum, up_sum, sgu, pre, pre_other, hidden, shared,
    wd, half_send, half_recv, total, held, sdh, part, red_send, red_recv, far_send, far_recv, row_send, row_recv,
    w_sem, k_send, k_recv, h_send, h_recv, x_send, x_recv, o_send, o_recv, r_send, r_recv, q_send, q_recv,
    g_send, g_recv, a_send, a_recv, f_send, f_recv, s_send, s_recv,
    d_send, d_recv, t_send, t_recv, b_send, b_recv, e_send, e_recv, m_send, m_recv, n_send, n_recv, z_send, z_recv,
):
    p = Place()
    c, nc = p.c, CHUNKS
    rows = queries.shape[1]
    my_rows, width = residual.shape
    half = width // 2
    fc = half // nc
    head_rows = w_out.shape[0]
    chip_rows = 2 * my_rows
    blocks = rows // WINDOW
    experts = p.sp_count * p.nz
    slots = pick.shape[0]
    capacity = slots // p.sp_count
    units = sg.shape[0]
    tile = min(256, rows, slots)
    last = p.nz // 2
    everything = tuple(range(nc))
    kv = p.t // GROUP
    kv_cols = pl.ds(pl.multiple_of(kv // 2 * 128, 128), 128)
    f32, bf = jnp.float32, jnp.bfloat16

    def half_of(h):
        return pl.ds(pl.multiple_of(h * half, half), half)

    def cols(h, j):
        return pl.ds(pl.multiple_of(h * half + j * fc, fc), fc)

    pairs = ((wg_hbm, wg), (wu_hbm, wu), (wd_hbm, wd))
    fetches = [pltpu.make_async_copy(src, dst, w_sem.at[i]) for i, (src, dst) in enumerate(pairs)]
    for copy in fetches:
        copy.start()
    p.barrier()

    def shard(core):
        return pl.ds(pl.multiple_of(p.z * 2 * head_rows + core * head_rows, head_rows), head_rows)

    def swap(j, core):
        return remote(
            w_out.at[:, cols(1 - c, j)], wide.at[j, shard(core)], x_send.at[j], x_recv.at[j], p.partner
        )

    rim = pl.ds(rows - WINDOW, WINDOW)
    following = ((p.s + 1) % p.sp_count, p.t)
    halo = [
        remote(ref.at[rim, kv_cols], ext.at[pl.ds(0, WINDOW)], k_send.at[i], k_recv.at[i], following)
        for i, (ref, ext) in enumerate(((keys, key_ext), (values, value_ext)))
    ]
    sends_rim, gets_rim = p.s + 1 < p.sp_count, p.s > 0

    def part_of(core):
        return pl.ds(pl.multiple_of(core * my_rows, my_rows), my_rows)

    def swap_res(core):
        return remote(residual.at[:, half_of(1 - c)], res.at[part_of(core)], r_send.at[0], r_recv.at[0], p.partner)

    unit_rows = [pl.ds(pl.multiple_of(k * 2 * units + c * units, units), units) for k in range(2)]
    my_units = pl.ds(pl.multiple_of(c * units, units), units)
    shared_swaps = [
        remote(sg.at[:, half_of(1 - c)], sgu.at[unit_rows[0]], s_send.at[0], s_recv.at[0], p.partner),
        remote(su.at[:, half_of(1 - c)], sgu.at[unit_rows[1]], s_send.at[1], s_recv.at[1], p.partner),
        remote(sd.at[:, half_of(1 - c)], sdh.at[my_units], d_send.at[0], d_recv.at[0], p.partner),
    ]
    for j in everything:
        swap(j, c).start()

    @pl.when(sends_rim)
    def _():
        for copy in halo:
            copy.start()

    swap_res(c).start()
    for copy in shared_swaps:
        copy.start()
    for j in everything:
        wide[j, shard(c)] = w_out[:, cols(c, j)]
    ring = RingGather(p, wide, 2 * head_rows, o_send, o_recv)
    for j in everything:
        swap(j, 1 - c).wait_recv()
        ring.send(j, 1)
    hops = iter([(j, k) for k in range(1, last) for j in everything])

    def hop(count=1):
        for _ in range(count):
            event = next(hops, None)
            if event is not None:
                ring.wait(*event)
                ring.send(event[0], event[1] + 1)

    key_ext[pl.ds(WINDOW, rows)] = keys[:, kv_cols]
    value_ext[pl.ds(WINDOW, rows)] = values[:, kv_cols]
    res[part_of(c)] = residual[:, half_of(c)]
    sgu[unit_rows[0]] = sg[:, half_of(c)]
    sgu[unit_rows[1]] = su[:, half_of(c)]
    sdh[my_units] = sd[:, half_of(c)]

    @pl.when(gets_rim)
    def _():
        for copy in halo:
            copy.wait_recv()

    @pl.when(jnp.logical_not(gets_rim))
    def _():
        key_ext[pl.ds(0, WINDOW)] = jnp.zeros((WINDOW, 128), bf)
        value_ext[pl.ds(0, WINDOW)] = jnp.zeros((WINDOW, 128), bf)

    lane_half = kv % 2
    sink_value = sink[...]
    head_place = pl.ds(pl.multiple_of(p.t * HD, HD), HD)

    def head_piece(b, device):
        return remote(att.at[b], heads.at[head_place], h_send.at[0], h_recv.at[0], device)

    others = heads.at[pl.ds(0, (p.tp_count - 1) * HD)]
    head_total = remote(others, others, h_send.at[0], h_recv.at[0], p.partner)

    def attend(i):
        b = (p.z + i) % blocks
        here = pl.ds(pl.multiple_of(b * WINDOW, WINDOW), WINDOW)
        ext = pl.ds(pl.multiple_of(b * WINDOW, WINDOW), 2 * WINDOW)
        query = queries[:, here].astype(f32)
        query = jnp.concatenate([query, query], axis=0)
        in_half = jnp.right_shift(iota((2 * HD, WINDOW), 0), HD.bit_length() - 1) == lane_half
        query = jnp.where(in_half, query, 0.0).astype(bf)
        scores = dot_nn(key_ext[ext], query) * HD ** (-0.5)
        key_pos = iota((2 * WINDOW, WINDOW), 0)
        query_pos = iota((2 * WINDOW, WINDOW), 1) + WINDOW
        first_key = jnp.where(p.s * blocks + b == 0, WINDOW, 0)
        allowed = (key_pos <= query_pos) & (key_pos > query_pos - WINDOW) & (key_pos >= first_key)
        scores = jnp.where(allowed, scores, -jnp.inf)
        top = jnp.maximum(jnp.max(scores, axis=0, keepdims=True), sink_value)
        exps = jnp.exp(scores - top)
        full = jnp.sum(exps, axis=0, keepdims=True) + jnp.exp(sink_value - top)
        shares = (exps / full).astype(bf)
        both = lax.dot_general(
            value_ext[ext], shares, (((0,), (0,)), ((), ())), preferred_element_type=f32
        )
        att[b] = jnp.where(lane_half == 0, both[:HD], both[HD:]).astype(bf)
        for core in range(2):
            target = 2 * b + core

            @pl.when(target != p.t)
            def _():
                head_piece(b, (p.s, target)).start()

            @pl.when(target == p.t)
            def _():
                heads[head_place] = att[b]

    def attend_some(first, count):
        def one(i, carry):
            attend(i)
            return carry

        lax.fori_loop(first, first + count, one, 0)

    quarter = max(1, blocks // 4)
    for i in range(0, blocks, quarter):
        attend_some(i, quarter)
        hop(1 if i == 0 else 2)

    shift = capacity.bit_length() - 1

    def name_rows(i, carry):
        span = pl.ds(pl.multiple_of(i * tile, tile), tile)
        expert = iota((experts, tile), 0)
        named = jnp.zeros((experts, tile), f32)
        weight = jnp.zeros((experts, tile), f32)
        tile_ids, tile_weights = ids[:, span], weights[:, span]
        for k in range(TOPK):
            same = tile_ids[k : k + 1] == expert
            named = jnp.where(same, 1.0, named)
            weight = jnp.where(same, tile_weights[k : k + 1], weight)
        rank_t[:, span] = named.astype(bf)
        weight_buf[span] = weight.T.astype(bf)
        return carry

    lax.fori_loop(0, rows // tile, name_rows, 0)
    hop()
    all_named = rank_t[...]
    ranks = []
    for i in range(rows // tile):
        before = iota((rows, tile), 0) < iota((rows, tile), 1) + i * tile
        rank = dot_nn(all_named, jnp.where(before, 1.0, 0.0).astype(bf))
        named = all_named[:, i * tile : (i + 1) * tile].astype(f32) > 0.0
        ranks.append(jnp.where(named, rank, -1.0))
    for i, rank in enumerate(ranks):
        rank_t[:, i * tile : (i + 1) * tile] = rank.astype(bf)
        rank_buf[i * tile : (i + 1) * tile] = rank.T.astype(bf)
    hop()

    def holds(first, count):
        slot = iota((count, experts), 0) + first
        same = jnp.right_shift(slot, shift) * p.nz + p.z == iota((count, experts), 1)
        return jnp.where(same, 1.0, 0.0).astype(bf)

    def fill_pick(r, first):
        place = jnp.bitwise_and(iota((tile, rows), 0) + first, capacity - 1).astype(f32)
        hit = dot_nn(holds(first, tile), rank_t[...]) == place
        pick[r] = jnp.where(hit, 1.0, 0.0).astype(bf)

    for i in range(slots // tile):
        fill_pick(pl.ds(i * tile, tile), i * tile)
        hop()

    def fill_blend(r):
        all_holds = holds(0, slots)
        place = jnp.bitwise_and(iota((tile, slots), 1), capacity - 1).astype(f32)
        hit = dot_nt(rank_buf[r], all_holds) == place
        blend[r] = jnp.where(hit, dot_nt(weight_buf[r], all_holds), 0.0).astype(bf)

    def fill_blend_tiles(first, end):
        for i in range(first, end):
            fill_blend(pl.ds(i * tile, tile))

    hop(nc * last)

    head_total.wait_recv()
    heads_t[...] = heads[...].T
    swap_res(1 - c).wait_recv()
    chip_place = pl.ds(pl.multiple_of(p.z * chip_rows, chip_rows), chip_rows)
    gather = RingGather(p, ring_buf, chip_rows, g_send, g_recv)
    squares = jnp.zeros((chip_rows, 1), f32)
    for j in everything:
        ring.wait(j, last)
        piece = pl.ds(j * fc, fc)
        mixed = (res[:, piece].astype(f32) + dot_nn(heads_t[...], wide[j])).astype(bf)
        after[:, piece] = mixed
        ring_buf[j, chip_place] = mixed
        gather.send(j, 1)
        mixed = mixed.astype(f32)
        squares = squares + jnp.sum(mixed * mixed, axis=1, keepdims=True)
    square[...] = jnp.broadcast_to(squares, square.shape)
    swap_square = remote(square, square_other, q_send.at[0], q_recv.at[0], p.partner)
    swap_square.start()
    fill_blend_tiles(0, 1)
    swap_square.wait_recv()
    mean = (square[...] + square_other[...]) / width
    scale_rows[p.z] = lax.rsqrt(mean + 1e-06).T[:8]

    def send_scale(o):
        mine = scale_rows.at[p.z]
        return remote(mine, mine, n_send.at[0], n_recv.at[0], (p.s, (p.t + 2 * o) % p.tp_count))

    for o in range(1, p.nz):
        send_scale(o).start()
    all_scales = scale_rows.at[pl.ds(0, p.nz - 1)]
    scale_total = remote(all_scales, all_scales, n_send.at[0], n_recv.at[0], p.partner)

    def take_scales():
        scale_total.wait_recv()
        for z in range(p.nz):
            block = jnp.broadcast_to(scale_rows[z, :1], (128, chip_rows))
            scale_cols[z * chip_rows : (z + 1) * chip_rows] = block.T
        flat = jnp.concatenate([scale_rows[z, :1] for z in range(p.nz)], axis=1)

        def one(r):
            found = jnp.sum(pick[r].astype(f32) * flat, axis=1, keepdims=True)
            scale_slots[r] = jnp.broadcast_to(found, (tile, 128))

        rows_loop(slots, tile, one)

    even = [pl.ds(j * fc, fc) for j in everything]
    spread = Exchange(p, outgoing, own, capacity, even, a_send, a_recv)

    def forward(j):
        return remote(own.at[:, even[j]], other.at[:, even[j]], f_send.at[j], f_recv.at[j], p.partner)

    def pass_on(pair, k):
        for j in pair:
            gather.wait(j, k)
            gather.send(j, k + 1)

    def select(j):
        gather.wait(j, last)

        def one(r):
            value = dot_nn(pick[r], ring_buf[j]) * scale_slots[r][:, :1] * gain[:, cols(c, j)]
            outgoing[r, even[j]] = value.astype(bf)

        rows_loop(slots, tile, one)
        spread.send(j)

    def shared_part(j):
        def one(r):
            normed = ring_buf[j, r].astype(f32) * scale_cols[r][:, :1] * gain[:, cols(c, j)]
            value = dot_nt(normed.astype(bf), sgu[:, j * fc : (j + 1) * fc])
            pre[r] = value if j == 0 else pre[r] + value

        rows_loop(rows, tile, one)

    def arrive(j):
        spread.wait(j)
        forward(j).start()

    def multiply(j):
        forward(j).wait_recv()

        def one(r):
            a, b = own[r, even[j]], other[r, even[j]]
            for w, acc in ((wg, gate_sum), (wu, up_sum)):
                value = dot_nt(a, w[:, cols(c, j)]) + dot_nt(b, w[:, cols(1 - c, j)])
                acc[r] = value if j == 0 else acc[r] + value

        rows_loop(slots, tile, one)

    for k in range(1, last):
        pass_on(everything, k)
        if k == 1:
            fill_blend_tiles(1, rows // tile)
            take_scales()
    if last == 1:
        fill_blend_tiles(1, rows // tile)
        take_scales()
    for copy in shared_swaps:
        copy.wait_recv()
    for j in everything:
        select(j)
    for j in (0, 1):
        shared_part(j)
    arrive(0)
    for copy in fetches[:2]:
        copy.wait()
    multiply(0)
    for j in (2, 3):
        shared_part(j)
    swap_pre = remote(pre, pre_other, s_send.at[2], s_recv.at[2], p.partner)
    swap_pre.start()
    arrive(1)
    swap_pre.wait_recv()

    def shared_one(r):
        both = pre[r] + pre_other[r]
        shared[r] = silu_times(both[:, : 2 * units], both[:, 2 * units :])

    rows_loop(rows, tile, shared_one)
    multiply(1)
    arrive(2)
    multiply(2)
    arrive(3)
    multiply(3)

    def hidden_one(r):
        hidden[r] = silu_times(gate_sum[r], up_sum[r])

    rows_loop(slots, tile, hidden_one)

    fetches[2].wait()
    unit = half // sum(CUTS)
    starts = [sum(CUTS[:j]) * unit for j in range(len(CUTS))]
    sizes = [cut * unit for cut in CUTS]
    spans = [pl.ds(a, n) for a, n in zip(starts, sizes)]
    count = len(CUTS)
    back = Exchange(p, total, held, capacity, spans, b_send, b_recv)

    def span_of(h, j):
        return pl.ds(pl.multiple_of(h * half + starts[j], unit), sizes[j])

    def give(j):
        return remote(half_send.at[:, spans[j]], half_recv.at[:, spans[j]], t_send.at[j], t_recv.at[j], p.partner)

    def down(j):
        def theirs(r):
            half_send[r, spans[j]] = dot_nn(hidden[r], wd[:, span_of(1 - c, j)]).astype(bf)

        def ours(r):
            total[r, spans[j]] = dot_nn(hidden[r], wd[:, span_of(c, j)]).astype(bf)

        rows_loop(slots, tile, theirs)
        give(j).start()
        rows_loop(slots, tile, ours)

    def add_halves(j):
        give(j).wait_recv()

        def one(r):
            both = total[r, spans[j]].astype(f32) + half_recv[r, spans[j]].astype(f32)
            total[r, spans[j]] = both.astype(bf)

        rows_loop(slots, tile, one)
        back.send(j)

    def blend_rows(j):
        back.wait(j)

        def one(r):
            mixed = dot_nn(blend[r], held[:, spans[j]])
            part[r, spans[j]] = mixed + dot_nn(shared[r], sdh[:, spans[j]])

        rows_loop(rows, tile, one)

    def chip_block(distance):
        index = (p.z + distance + p.nz) % p.nz
        return pl.ds(pl.multiple_of(index * chip_rows, chip_rows), chip_rows)

    def red(j, way, m):
        sems = e_send.at[j, way, m - 1], e_recv.at[j, way, m - 1]
        refs = [ref.at[way, m - 1, :, spans[j]] for ref in (red_send, red_recv)]
        return remote(*refs, *sems, p.left if way else p.right)

    def step(j, m):
        for way in range(2):
            n = p.steps(j)[way]
            if m > n:
                continue
            distance = n - m + 1
            value = part[chip_block(-distance if way else distance), spans[j]]
            if m > 1:
                red(j, way, m - 1).wait_recv()
                value = value + red_recv[way, m - 2, :, spans[j]].astype(f32)
            red_send[way, m - 1, :, spans[j]] = value.astype(bf)
            red(j, way, m).start()

    def far(o):
        device = (p.s, (p.t + 2 * o) % p.tp_count)
        return remote(far_send.at[o - 1], far_recv.at[o - 1], z_send.at[o - 1], z_recv.at[o - 1], device)

    def send_far(j):
        for o in (o for o in sorted(range(1, p.nz), key=lambda o: -min(o, p.nz - o))):
            far_send[o - 1] = part[chip_block(o), spans[j]].astype(bf)
            far(o).start()

    def give_rows(j):
        return remote(row_send.at[:, spans[j]], row_recv.at[:, spans[j]], m_send.at[j], m_recv.at[j], p.partner)

    def finish(j):
        ends = []
        if j == count - 1:
            for o in range(1, p.nz):
                far(o).wait_recv()
                ends.append(far_recv.at[o - 1])
        else:
            for way in range(2):
                n = p.steps(j)[way]
                if n:
                    red(j, way, n).wait_recv()
                    ends.append(red_recv.at[way, n - 1, :, spans[j]])

        def layer_rows(core):
            base = pl.ds(pl.multiple_of(p.z * chip_rows + core * my_rows, my_rows), my_rows)
            value = part[base, spans[j]]
            for end in ends:
                value = value + end[part_of(core)].astype(f32)
            moe = value.astype(bf).astype(f32)
            return (after[part_of(core), spans[j]].astype(f32) + moe).astype(bf)

        row_send[:, spans[j]] = layer_rows(1 - c)
        give_rows(j).start()
        out[:, span_of(c, j)] = layer_rows(c)

    def take_rows(j):
        give_rows(j).wait_recv()
        out[:, span_of(1 - c, j)] = row_recv[:, spans[j]]

    down(0)
    for j in range(1, count):
        down(j)
        add_halves(j - 1)
    add_halves(count - 1)
    at = {}

    def advance():
        for j in sorted(at):
            if j == count - 1:
                if at[j] == 1:
                    send_far(j)
                elif at[j] == last:
                    finish(j)
            elif at[j] <= last:
                step(j, at[j])
            elif at[j] == last + 1:
                finish(j)
            at[j] += 1

    for j in range(count):
        blend_rows(j)
        at[j] = 1
        advance()
    while min(at[count - 1] + 1, at[count - 2]) <= last + 1:
        advance()
    for j in range(count):
        take_rows(j)

    @pl.when(sends_rim)
    def _():
        for copy in halo:
            copy.wait_send()

    for j in everything:
        swap(j, c).wait_send()
        ring.drain(j)
        gather.drain(j)
        spread.drain(j)
        forward(j).wait_send()
    swap_res(c).wait_send()
    head_total.wait_send()
    swap_square.wait_send()
    for copy in shared_swaps:
        copy.wait_send()
    swap_pre.wait_send()
    for j in range(count):
        give(j).wait_send()
        back.drain(j)
        give_rows(j).wait_send()
        for way in range(2):
            for m in range(1, p.steps(j)[way] + 1 if j < count - 1 else 1):
                red(j, way, m).wait_send()
    scale_total.wait_send()
    for o in range(1, p.nz):
        far(o).wait_send()


def vmem():
    return pl.BlockSpec(memory_space=pltpu.VMEM)


def layer(queries, keys, values, sink, w_out, residual, gain, ids, weights, wg, wu, wd, sg, su, sd):
    nc, cuts = CHUNKS, len(CUTS)
    rows = queries.shape[1]
    my_rows, width = residual.shape
    half, chip_rows = width // 2, 2 * my_rows
    fc = half // nc
    tp_count, sp_count = lax.axis_size("tp"), lax.axis_size("sp")
    experts = sp_count * tp_count // 2
    slots = sp_count * CAP
    hops = tp_count // 4
    hidden_units, units = wg.shape[0], sg.shape[0]
    bf, f32 = jnp.bfloat16, jnp.float32

    def buf(*shape, dtype=bf):
        return pltpu.VMEM(shape, dtype)

    def sems(*shape):
        return [pltpu.SemaphoreType.DMA(shape)] * 2

    anywhere = pl.BlockSpec(memory_space=pl.ANY)
    return pl.pallas_call(
        layer_kernel,
        name="layer",
        out_shape=jax.ShapeDtypeStruct((my_rows, width), bf),
        in_specs=[vmem()] * 9 + [anywhere] * 3 + [vmem()] * 3,
        out_specs=vmem(),
        scratch_shapes=[
            buf(rows + WINDOW, 128),
            buf(rows + WINDOW, 128),
            buf(rows // WINDOW, HD, WINDOW),
            buf(tp_count * HD, chip_rows),
            buf(chip_rows, tp_count * HD),
            buf(nc, tp_count * HD, fc),
            buf(chip_rows, half),
            buf(chip_rows, half),
            buf(chip_rows, 128, dtype=f32),
            buf(chip_rows, 128, dtype=f32),
            buf(rows, experts),
            buf(experts, rows),
            buf(rows, experts),
            buf(slots, rows),
            buf(rows, slots),
            buf(tp_count // 2, 8, chip_rows, dtype=f32),
            buf(rows, 128, dtype=f32),
            buf(slots, 128, dtype=f32),
            buf(nc, rows, fc),
            buf(slots, half),
            buf(slots, half),
            buf(slots, half),
            buf(hidden_units, width),
            buf(hidden_units, width),
            buf(slots, hidden_units, dtype=f32),
            buf(slots, hidden_units, dtype=f32),
            buf(4 * units, half),
            buf(rows, 4 * units, dtype=f32),
            buf(rows, 4 * units, dtype=f32),
            buf(slots, hidden_units),
            buf(rows, 2 * units),
            buf(hidden_units, width),
            buf(slots, half),
            buf(slots, half),
            buf(slots, half),
            buf(slots, half),
            buf(2 * units, half),
            buf(rows, half, dtype=f32),
            buf(2, hops, chip_rows, half),
            buf(2, hops, chip_rows, half),
            buf(tp_count // 2 - 1, chip_rows, half // sum(CUTS) * CUTS[-1]),
            buf(tp_count // 2 - 1, chip_rows, half // sum(CUTS) * CUTS[-1]),
            buf(my_rows, half),
            buf(my_rows, half),
            pltpu.SemaphoreType.DMA((3,)),
            *sems(2),
            *sems(1),
            *sems(nc),
            *sems(nc, 2, hops),
            *sems(1),
            *sems(1),
            *sems(nc, 2, hops),
            *sems(nc),
            *sems(nc),
            *sems(3),
            *sems(1),
            *sems(cuts),
            *sems(cuts),
            *sems(cuts, 2, hops),
            *sems(cuts),
            *sems(1),
            *sems(tp_count // 2 - 1),
        ],
        compiler_params=pltpu.CompilerParams(
            collective_id=1, has_side_effects=True, vmem_limit_bytes=66_000_000
        ),
    )(queries, keys, values, sink, w_out, residual, gain, ids, weights, wg, wu, wd, sg, su, sd)


def body(
    queries,
    keys,
    values,
    sink_logits,
    w_out,
    residual,
    norm_gain,
    expert_ids,
    expert_weights,
    w_gate,
    w_up,
    w_down,
    shared_gate,
    shared_up,
    shared_down,
):
    return layer(
        queries.T,
        keys,
        values,
        sink_logits[:, None],
        w_out,
        residual,
        norm_gain[None, :],
        expert_ids.T,
        expert_weights.T,
        w_gate[0],
        w_up[0],
        w_down[0],
        shared_gate,
        shared_up,
        shared_down,
    )


def solution(mesh):
    return jax.shard_map(
        body,
        mesh=mesh,
        in_specs=(
            P("sp", "tp"),
            P("sp", None),
            P("sp", None),
            P("tp"),
            P("tp", None),
            P(("sp", "tp"), None),
            P(),
            P("sp", None),
            P("sp", None),
            P(("sp", "tp"), None, None),
            P(("sp", "tp"), None, None),
            P(("sp", "tp"), None, None),
            P("tp", None),
            P("tp", None),
            P("tp", None),
        ),
        out_specs=P(("sp", "tp"), None),
        check_vma=False,
    )
```

```python
import jax
import jax.numpy as jnp
from jax import lax
from jax.experimental import pallas as pl
from jax.experimental.pallas import tpu as pltpu
from jax.sharding import PartitionSpec as P

HD = 64
GROUP = 4
WINDOW = 128
TOPK = 4


MESH = pl.DeviceIdType.MESH
CHUNKS = 4
TALL = 512
FAR = True
CUTS = (2, 2, 2, 1, 1)
CAP = 64


def dot_nt(a, b):
    return lax.dot_general(a, b, (((1,), (1,)), ((), ())), preferred_element_type=jnp.float32)


def dot_nn(a, b):
    return jnp.dot(a, b, preferred_element_type=jnp.float32)


def rows_loop(total, step, fn):
    def one(i, carry):
        fn(pl.ds(pl.multiple_of(i * step, step), step))
        return carry

    lax.fori_loop(0, total // step, one, 0)


class Place:
    def __init__(self):
        self.sp_count = lax.axis_size("sp")
        self.tp_count = lax.axis_size("tp")
        self.s = lax.axis_index("sp")
        self.t = lax.axis_index("tp")
        self.c = self.t % 2
        self.z = self.t // 2
        self.nz = self.tp_count // 2
        self.partner = (self.s, self.t + 1 - 2 * self.c)
        self.right = (self.s, (self.t + 2) % self.tp_count)
        self.left = (self.s, (self.t + self.tp_count - 2) % self.tp_count)

    def peer(self, o):
        return ((self.s + o) % self.sp_count, self.t)

    def barrier(self):
        sem = pltpu.get_barrier_semaphore()

        def greet(count, device):
            def one(o, carry):
                pl.semaphore_signal(sem, inc=1, device_id=device(o), device_id_type=MESH)
                return carry

            lax.fori_loop(1, count, one, 0)

        greet(self.tp_count, lambda o: (self.s, (self.t + o) % self.tp_count))
        greet(self.sp_count, self.peer)
        pl.semaphore_wait(sem, self.tp_count + self.sp_count - 2)

    def steps(self, j):
        far, near = self.nz // 2, self.nz - 1 - self.nz // 2
        return (far, near) if j % 2 == 0 else (near, far)


def remote(src, dst, send_sem, recv_sem, device):
    return pltpu.make_async_remote_copy(
        src_ref=src, dst_ref=dst, send_sem=send_sem, recv_sem=recv_sem, device_id=device, device_id_type=MESH
    )


class RingGather:
    def __init__(self, p, buf, rows, send_sems, recv_sems):
        self.p, self.buf, self.rows = p, buf, rows
        self.ss, self.rs = send_sems, recv_sems

    def copy(self, j, way, k, shift):
        p = self.p
        origin = (p.z - shift if way == 0 else p.z + shift) + p.nz
        block = self.buf.at[j, pl.ds(pl.multiple_of(origin % p.nz * self.rows, self.rows), self.rows)]
        return remote(block, block, self.ss.at[j, way, k - 1], self.rs.at[j, way, k - 1], p.left if way else p.right)

    def send(self, j, k):
        for way in range(2):
            if k <= self.p.steps(j)[way]:
                self.copy(j, way, k, k - 1).start()

    def wait(self, j, k):
        for way in range(2):
            if k <= self.p.steps(j)[way]:
                self.copy(j, way, k, k).wait_recv()

    def drain(self, j):
        for way in range(2):
            for k in range(1, self.p.steps(j)[way] + 1):
                self.copy(j, way, k, k - 1).wait_send()


class Exchange:
    def __init__(self, p, src, dst, rows, spans, send_sems, recv_sems):
        self.p, self.src, self.dst, self.rows, self.spans = p, src, dst, rows, spans
        self.ss, self.rs = send_sems, recv_sems

    def block(self, index, j):
        return pl.ds(pl.multiple_of(index * self.rows, self.rows), self.rows), self.spans[j]

    def send(self, j):
        p = self.p

        def one(o, carry):
            peer = p.peer(o)
            remote(
                self.src.at[self.block(peer[0], j)],
                self.dst.at[self.block(p.s, j)],
                self.ss.at[j],
                self.rs.at[j],
                peer,
            ).start()
            return carry

        lax.fori_loop(1, p.sp_count, one, 0)
        self.dst[self.block(p.s, j)] = self.src[self.block(p.s, j)]

    def all_of(self, j):
        others = pl.ds(0, (self.p.sp_count - 1) * self.rows), self.spans[j]
        return remote(self.src.at[others], self.dst.at[others], self.ss.at[j], self.rs.at[j], self.p.peer(1))

    def wait(self, j):
        self.all_of(j).wait_recv()

    def drain(self, j):
        self.all_of(j).wait_send()


def iota(shape, axis):
    return lax.broadcasted_iota(jnp.int32, shape, axis)


def silu_times(gate, up):
    return (gate / (1.0 + jnp.exp(-gate)) * up).astype(jnp.bfloat16)


def layer_kernel(
    queries, keys, values, sink, w_out, residual, gain, ids, weights, wg_hbm, wu_hbm, wd_hbm, sg, su, sd,
    out,
    key_ext, value_ext, att, heads, heads_t, wide, res, after, square, square_other,
    rank_buf, rank_t, weight_buf, pick, blend, scale_rows, scale_cols, scale_slots,
    ring_buf, outgoing, own, other, wg, wu, gate_sum, up_sum, sgu, pre, pre_other, hidden, shared,
    wd, half_send, half_recv, total, held, sdh, part, red_send, red_recv, far_send, far_recv, row_send, row_recv,
    w_sem, k_send, k_recv, h_send, h_recv, x_send, x_recv, o_send, o_recv, r_send, r_recv, q_send, q_recv,
    g_send, g_recv, a_send, a_recv, f_send, f_recv, s_send, s_recv,
    d_send, d_recv, t_send, t_recv, b_send, b_recv, e_send, e_recv, m_send, m_recv, n_send, n_recv, z_send, z_recv,
):
    p = Place()
    c, nc = p.c, CHUNKS
    rows = queries.shape[1]
    my_rows, width = residual.shape
    half = width // 2
    fc = half // nc
    head_rows = w_out.shape[0]
    chip_rows = 2 * my_rows
    blocks = rows // WINDOW
    experts = p.sp_count * p.nz
    slots = pick.shape[0]
    capacity = slots // p.sp_count
    units = sg.shape[0]
    tile = min(256, rows, slots)
    tall = min(TALL, rows, slots)
    last = p.nz // 2
    everything = tuple(range(nc))
    kv = p.t // GROUP
    kv_cols = pl.ds(pl.multiple_of(kv // 2 * 128, 128), 128)
    f32, bf = jnp.float32, jnp.bfloat16

    def half_of(h):
        return pl.ds(pl.multiple_of(h * half, half), half)

    def cols(h, j):
        return pl.ds(pl.multiple_of(h * half + j * fc, fc), fc)

    pairs = ((wg_hbm, wg), (wu_hbm, wu), (wd_hbm, wd))
    fetches = [pltpu.make_async_copy(src, dst, w_sem.at[i]) for i, (src, dst) in enumerate(pairs)]
    for copy in fetches:
        copy.start()
    p.barrier()

    def shard(core):
        return pl.ds(pl.multiple_of(p.z * 2 * head_rows + core * head_rows, head_rows), head_rows)

    def swap(j, core):
        return remote(
            w_out.at[:, cols(1 - c, j)], wide.at[j, shard(core)], x_send.at[j], x_recv.at[j], p.partner
        )

    rim = pl.ds(rows - WINDOW, WINDOW)
    following = ((p.s + 1) % p.sp_count, p.t)
    halo = [
        remote(ref.at[rim, kv_cols], ext.at[pl.ds(0, WINDOW)], k_send.at[i], k_recv.at[i], following)
        for i, (ref, ext) in enumerate(((keys, key_ext), (values, value_ext)))
    ]
    sends_rim, gets_rim = p.s + 1 < p.sp_count, p.s > 0

    def part_of(core):
        return pl.ds(pl.multiple_of(core * my_rows, my_rows), my_rows)

    def swap_res(core):
        return remote(residual.at[:, half_of(1 - c)], res.at[part_of(core)], r_send.at[0], r_recv.at[0], p.partner)

    unit_rows = [pl.ds(pl.multiple_of(k * 2 * units + c * units, units), units) for k in range(2)]
    my_units = pl.ds(pl.multiple_of(c * units, units), units)
    shared_swaps = [
        remote(sg.at[:, half_of(1 - c)], sgu.at[unit_rows[0]], s_send.at[0], s_recv.at[0], p.partner),
        remote(su.at[:, half_of(1 - c)], sgu.at[unit_rows[1]], s_send.at[1], s_recv.at[1], p.partner),
        remote(sd.at[:, half_of(1 - c)], sdh.at[my_units], d_send.at[0], d_recv.at[0], p.partner),
    ]
    for j in everything:
        swap(j, c).start()

    @pl.when(sends_rim)
    def _():
        for copy in halo:
            copy.start()

    swap_res(c).start()
    for copy in shared_swaps:
        copy.start()
    for j in everything:
        wide[j, shard(c)] = w_out[:, cols(c, j)]
    ring = RingGather(p, wide, 2 * head_rows, o_send, o_recv)
    first, second = (0, 1), (2, 3)
    turns = sorted([(2 * k, first, k) for k in range(last)] + [(2 * k + 3, second, k) for k in range(last)])
    hops = [(j, k) for _, pair, k in turns for j in pair]

    def hop(count=1):
        for _ in range(min(count, len(hops))):
            j, k = hops.pop(0)
            if k:
                ring.wait(j, k)
            else:
                swap(j, 1 - c).wait_recv()
            ring.send(j, k + 1)

    hop(2)
    key_ext[pl.ds(WINDOW, rows)] = keys[:, kv_cols]
    value_ext[pl.ds(WINDOW, rows)] = values[:, kv_cols]
    res[part_of(c)] = residual[:, half_of(c)]
    sgu[unit_rows[0]] = sg[:, half_of(c)]
    sgu[unit_rows[1]] = su[:, half_of(c)]
    sdh[my_units] = sd[:, half_of(c)]

    @pl.when(gets_rim)
    def _():
        for copy in halo:
            copy.wait_recv()

    @pl.when(jnp.logical_not(gets_rim))
    def _():
        key_ext[pl.ds(0, WINDOW)] = jnp.zeros((WINDOW, 128), bf)
        value_ext[pl.ds(0, WINDOW)] = jnp.zeros((WINDOW, 128), bf)

    lane_half = kv % 2
    sink_value = sink[...]
    head_place = pl.ds(pl.multiple_of(p.t * HD, HD), HD)

    def head_piece(b, device):
        return remote(att.at[b], heads.at[head_place], h_send.at[0], h_recv.at[0], device)

    others = heads.at[pl.ds(0, (p.tp_count - 1) * HD)]
    head_total = remote(others, others, h_send.at[0], h_recv.at[0], p.partner)

    def attend(i):
        b = (p.z + i) % blocks
        here = pl.ds(pl.multiple_of(b * WINDOW, WINDOW), WINDOW)
        ext = pl.ds(pl.multiple_of(b * WINDOW, WINDOW), 2 * WINDOW)
        query = queries[:, here].astype(f32)
        query = jnp.concatenate([query, query], axis=0)
        in_half = jnp.right_shift(iota((2 * HD, WINDOW), 0), HD.bit_length() - 1) == lane_half
        query = jnp.where(in_half, query, 0.0).astype(bf)
        scores = dot_nn(key_ext[ext], query) * HD ** (-0.5)
        key_pos = iota((2 * WINDOW, WINDOW), 0)
        query_pos = iota((2 * WINDOW, WINDOW), 1) + WINDOW
        first_key = jnp.where(p.s * blocks + b == 0, WINDOW, 0)
        allowed = (key_pos <= query_pos) & (key_pos > query_pos - WINDOW) & (key_pos >= first_key)
        scores = jnp.where(allowed, scores, -jnp.inf)
        top = jnp.maximum(jnp.max(scores, axis=0, keepdims=True), sink_value)
        exps = jnp.exp(scores - top)
        full = jnp.sum(exps, axis=0, keepdims=True) + jnp.exp(sink_value - top)
        shares = (exps / full).astype(bf)
        both = lax.dot_general(
            value_ext[ext], shares, (((0,), (0,)), ((), ())), preferred_element_type=f32
        )
        att[b] = jnp.where(lane_half == 0, both[:HD], both[HD:]).astype(bf)
        for core in range(2):
            target = 2 * b + core

            @pl.when(target != p.t)
            def _():
                head_piece(b, (p.s, target)).start()

            @pl.when(target == p.t)
            def _():
                heads[head_place] = att[b]

    def attend_some(first, count):
        def one(i, carry):
            attend(i)
            return carry

        lax.fori_loop(first, first + count, one, 0)

    quarter = max(1, blocks // 4)
    for i in range(0, blocks, quarter):
        attend_some(i, quarter)
        hop((1, 3, 2, 2)[i // quarter])

    shift = capacity.bit_length() - 1

    def name_rows(i, carry):
        span = pl.ds(pl.multiple_of(i * tile, tile), tile)
        expert = iota((experts, tile), 0)
        named = jnp.zeros((experts, tile), f32)
        weight = jnp.zeros((experts, tile), f32)
        tile_ids, tile_weights = ids[:, span], weights[:, span]
        for k in range(TOPK):
            same = tile_ids[k : k + 1] == expert
            named = jnp.where(same, 1.0, named)
            weight = jnp.where(same, tile_weights[k : k + 1], weight)
        rank_t[:, span] = named.astype(bf)
        weight_buf[span] = weight.T.astype(bf)
        return carry

    lax.fori_loop(0, rows // tile, name_rows, 0)
    hop()
    all_named = rank_t[...]
    ranks = []
    for i in range(rows // tile):
        before = iota((rows, tile), 0) < iota((rows, tile), 1) + i * tile
        rank = dot_nn(all_named, jnp.where(before, 1.0, 0.0).astype(bf))
        named = all_named[:, i * tile : (i + 1) * tile].astype(f32) > 0.0
        ranks.append(jnp.where(named, rank, -1.0))
    for i, rank in enumerate(ranks):
        rank_t[:, i * tile : (i + 1) * tile] = rank.astype(bf)
        rank_buf[i * tile : (i + 1) * tile] = rank.T.astype(bf)
    hop()

    def holds(first, count):
        slot = iota((count, experts), 0) + first
        same = jnp.right_shift(slot, shift) * p.nz + p.z == iota((count, experts), 1)
        return jnp.where(same, 1.0, 0.0).astype(bf)

    def fill_pick(r, first):
        place = jnp.bitwise_and(iota((tile, rows), 0) + first, capacity - 1).astype(f32)
        hit = dot_nn(holds(first, tile), rank_t[...]) == place
        pick[r] = jnp.where(hit, 1.0, 0.0).astype(bf)

    for i in range(slots // tile):
        fill_pick(pl.ds(i * tile, tile), i * tile)
        hop()

    def fill_blend(r):
        all_holds = holds(0, slots)
        place = jnp.bitwise_and(iota((tile, slots), 1), capacity - 1).astype(f32)
        hit = dot_nt(rank_buf[r], all_holds) == place
        blend[r] = jnp.where(hit, dot_nt(weight_buf[r], all_holds), 0.0).astype(bf)

    def fill_blend_tiles(first, end):
        for i in range(first, end):
            fill_blend(pl.ds(i * tile, tile))

    hop(len(hops) - 2)

    head_total.wait_recv()
    heads_t[...] = heads[...].T
    swap_res(1 - c).wait_recv()
    chip_place = pl.ds(pl.multiple_of(p.z * chip_rows, chip_rows), chip_rows)
    gather = RingGather(p, ring_buf, chip_rows, g_send, g_recv)

    def project(j):
        ring.wait(j, last)
        piece = pl.ds(j * fc, fc)
        mixed = (res[:, piece].astype(f32) + dot_nn(heads_t[...], wide[j])).astype(bf)
        after[:, piece] = mixed
        ring_buf[j, chip_place] = mixed
        gather.send(j, 1)
        mixed = mixed.astype(f32)
        return jnp.sum(mixed * mixed, axis=1, keepdims=True)

    def pass_on(pair, k):
        for j in pair if k < last else ():
            gather.wait(j, k)
            gather.send(j, k + 1)

    squares = project(0) + project(1)
    hop(2)
    pass_on(first, 1)
    squares = squares + project(2) + project(3)
    square[...] = jnp.broadcast_to(squares, square.shape)
    swap_square = remote(square, square_other, q_send.at[0], q_recv.at[0], p.partner)
    swap_square.start()
    pass_on(first, 2)
    swap_square.wait_recv()
    mean = (square[...] + square_other[...]) / width
    scale_rows[p.z] = lax.rsqrt(mean + 1e-06).T[:8]

    def send_scale(o):
        mine = scale_rows.at[p.z]
        return remote(mine, mine, n_send.at[0], n_recv.at[0], (p.s, (p.t + 2 * o) % p.tp_count))

    for o in range(1, p.nz):
        send_scale(o).start()
    all_scales = scale_rows.at[pl.ds(0, p.nz - 1)]
    scale_total = remote(all_scales, all_scales, n_send.at[0], n_recv.at[0], p.partner)

    def take_scales():
        scale_total.wait_recv()
        for z in range(p.nz):
            block = jnp.broadcast_to(scale_rows[z, :1], (128, chip_rows))
            scale_cols[z * chip_rows : (z + 1) * chip_rows] = block.T
        flat = jnp.concatenate([scale_rows[z, :1] for z in range(p.nz)], axis=1)

        def one(r):
            found = jnp.sum(pick[r].astype(f32) * flat, axis=1, keepdims=True)
            scale_slots[r] = jnp.broadcast_to(found, (tile, 128))

        rows_loop(slots, tile, one)

    even = [pl.ds(j * fc, fc) for j in everything]
    spread = Exchange(p, outgoing, own, capacity, even, a_send, a_recv)

    def forward(j):
        return remote(own.at[:, even[j]], other.at[:, even[j]], f_send.at[j], f_recv.at[j], p.partner)

    def select(j):
        gather.wait(j, last)

        def one(r):
            value = dot_nn(pick[r], ring_buf[j]) * scale_slots[r][:, :1] * gain[:, cols(c, j)]
            outgoing[r, even[j]] = value.astype(bf)

        rows_loop(slots, tall, one)
        spread.send(j)

    def shared_part(j):
        def one(r):
            normed = ring_buf[j, r].astype(f32) * scale_cols[r][:, :1] * gain[:, cols(c, j)]
            value = dot_nt(normed.astype(bf), sgu[:, j * fc : (j + 1) * fc])
            pre[r] = value if j == 0 else pre[r] + value

        rows_loop(rows, tile, one)

    def arrive(j):
        spread.wait(j)
        forward(j).start()

    def multiply(j):
        forward(j).wait_recv()

        def one(r):
            both = jnp.concatenate([own[r, even[j]], other[r, even[j]]], axis=1)
            for w, acc in ((wg, gate_sum), (wu, up_sum)):
                across = jnp.concatenate([w[:, cols(c, j)], w[:, cols(1 - c, j)]], axis=1)
                value = dot_nt(both, across)
                acc[r] = value if j == 0 else acc[r] + value

        rows_loop(slots, tall, one)

    fill_blend_tiles(0, rows // tile)
    pass_on(second, 1)
    pass_on(first, 3)
    for copy in shared_swaps:
        copy.wait_recv()
    pass_on(second, 2)
    take_scales()
    select(0)
    pass_on(second, 3)
    for j in (1, 2, 3):
        select(j)
    for j in (0, 1):
        shared_part(j)
    arrive(0)
    for copy in fetches[:2]:
        copy.wait()
    multiply(0)
    for j in (2, 3):
        shared_part(j)
    swap_pre = remote(pre, pre_other, s_send.at[2], s_recv.at[2], p.partner)
    swap_pre.start()
    arrive(1)
    swap_pre.wait_recv()

    def shared_one(r):
        both = pre[r] + pre_other[r]
        shared[r] = silu_times(both[:, : 2 * units], both[:, 2 * units :])

    rows_loop(rows, tile, shared_one)
    multiply(1)
    arrive(2)
    multiply(2)
    arrive(3)
    multiply(3)

    def hidden_one(r):
        hidden[r] = silu_times(gate_sum[r], up_sum[r])

    rows_loop(slots, tile, hidden_one)

    fetches[2].wait()
    unit = half // sum(CUTS)
    starts = [sum(CUTS[:j]) * unit for j in range(len(CUTS))]
    sizes = [cut * unit for cut in CUTS]
    spans = [pl.ds(a, n) for a, n in zip(starts, sizes)]
    count = len(CUTS)
    direct = count - 1 if FAR else None
    back = Exchange(p, total, held, capacity, spans, b_send, b_recv)

    def span_of(h, j):
        return pl.ds(pl.multiple_of(h * half + starts[j], unit), sizes[j])

    def give(j):
        return remote(half_send.at[:, spans[j]], half_recv.at[:, spans[j]], t_send.at[j], t_recv.at[j], p.partner)

    def down(j):
        def theirs(r):
            half_send[r, spans[j]] = dot_nn(hidden[r], wd[:, span_of(1 - c, j)]).astype(bf)

        def ours(r):
            total[r, spans[j]] = dot_nn(hidden[r], wd[:, span_of(c, j)]).astype(bf)

        rows_loop(slots, tall, theirs)
        give(j).start()
        rows_loop(slots, tall, ours)

    def add_halves(j):
        give(j).wait_recv()

        def one(r):
            both = total[r, spans[j]].astype(f32) + half_recv[r, spans[j]].astype(f32)
            total[r, spans[j]] = both.astype(bf)

        rows_loop(slots, tile, one)
        back.send(j)

    def blend_rows(j):
        back.wait(j)

        def one(r):
            mixed = dot_nn(blend[r], held[:, spans[j]])
            part[r, spans[j]] = mixed + dot_nn(shared[r], sdh[:, spans[j]])

        rows_loop(rows, tall, one)

    def chip_block(distance):
        index = (p.z + distance + p.nz) % p.nz
        return pl.ds(pl.multiple_of(index * chip_rows, chip_rows), chip_rows)

    def red(j, way, m):
        sems = e_send.at[j, way, m - 1], e_recv.at[j, way, m - 1]
        refs = [ref.at[way, m - 1, :, spans[j]] for ref in (red_send, red_recv)]
        return remote(*refs, *sems, p.left if way else p.right)

    def step(j, m):
        for way in range(2):
            n = p.steps(j)[way]
            if m > n:
                continue
            distance = n - m + 1
            value = part[chip_block(-distance if way else distance), spans[j]]
            if m > 1:
                red(j, way, m - 1).wait_recv()
                value = value + red_recv[way, m - 2, :, spans[j]].astype(f32)
            red_send[way, m - 1, :, spans[j]] = value.astype(bf)
            red(j, way, m).start()

    def far(o):
        device = (p.s, (p.t + 2 * o) % p.tp_count)
        return remote(far_send.at[o - 1], far_recv.at[o - 1], z_send.at[o - 1], z_recv.at[o - 1], device)

    def send_far(j):
        for o in sorted(range(1, p.nz), key=lambda o: -min(o, p.nz - o)):
            far_send[o - 1] = part[chip_block(o), spans[j]].astype(bf)
            far(o).start()

    def give_rows(j):
        return remote(row_send.at[:, spans[j]], row_recv.at[:, spans[j]], m_send.at[j], m_recv.at[j], p.partner)

    def finish(j):
        ends = []
        if j == direct:
            for o in range(1, p.nz):
                far(o).wait_recv()
                ends.append(far_recv.at[o - 1])
        else:
            for way in range(2):
                n = p.steps(j)[way]
                if n:
                    red(j, way, n).wait_recv()
                    ends.append(red_recv.at[way, n - 1, :, spans[j]])

        def layer_rows(core):
            base = pl.ds(pl.multiple_of(p.z * chip_rows + core * my_rows, my_rows), my_rows)
            value = part[base, spans[j]]
            for end in ends:
                value = value + end[part_of(core)].astype(f32)
            moe = value.astype(bf).astype(f32)
            return (after[part_of(core), spans[j]].astype(f32) + moe).astype(bf)

        row_send[:, spans[j]] = layer_rows(1 - c)
        give_rows(j).start()
        out[:, span_of(c, j)] = layer_rows(c)

    def take_rows(j):
        give_rows(j).wait_recv()
        out[:, span_of(1 - c, j)] = row_recv[:, spans[j]]

    down(0)
    for j in range(1, count):
        down(j)
        add_halves(j - 1)
    add_halves(count - 1)
    at = {}

    def advance():
        for j in sorted(at):
            if j == direct:
                if at[j] == 1:
                    send_far(j)
                elif at[j] == last:
                    finish(j)
            elif at[j] <= last:
                step(j, at[j])
            elif at[j] == last + 1:
                finish(j)
            at[j] += 1

    for j in range(count):
        blend_rows(j)
        at[j] = 1
        advance()
    while any(at[j] <= last + (j != direct) for j in at):
        advance()
    for j in range(count):
        take_rows(j)

    @pl.when(sends_rim)
    def _():
        for copy in halo:
            copy.wait_send()

    for j in everything:
        swap(j, c).wait_send()
        ring.drain(j)
        gather.drain(j)
        spread.drain(j)
        forward(j).wait_send()
    swap_res(c).wait_send()
    head_total.wait_send()
    swap_square.wait_send()
    for copy in shared_swaps:
        copy.wait_send()
    swap_pre.wait_send()
    for j in range(count):
        give(j).wait_send()
        back.drain(j)
        give_rows(j).wait_send()
        for way in range(2):
            for m in range(1, p.steps(j)[way] + 1 if j != direct else 1):
                red(j, way, m).wait_send()
    scale_total.wait_send()
    for o in range(1, p.nz if FAR else 1):
        far(o).wait_send()


def vmem():
    return pl.BlockSpec(memory_space=pltpu.VMEM)


def layer(queries, keys, values, sink, w_out, residual, gain, ids, weights, wg, wu, wd, sg, su, sd):
    nc, cuts = CHUNKS, len(CUTS)
    rows = queries.shape[1]
    my_rows, width = residual.shape
    half, chip_rows = width // 2, 2 * my_rows
    fc = half // nc
    tp_count, sp_count = lax.axis_size("tp"), lax.axis_size("sp")
    experts = sp_count * tp_count // 2
    slots = sp_count * CAP
    hops = tp_count // 4
    hidden_units, units = wg.shape[0], sg.shape[0]
    bf, f32 = jnp.bfloat16, jnp.float32

    def buf(*shape, dtype=bf):
        return pltpu.VMEM(shape, dtype)

    def sems(*shape):
        return [pltpu.SemaphoreType.DMA(shape)] * 2

    anywhere = pl.BlockSpec(memory_space=pl.ANY)
    return pl.pallas_call(
        layer_kernel,
        name="layer",
        out_shape=jax.ShapeDtypeStruct((my_rows, width), bf),
        in_specs=[vmem()] * 9 + [anywhere] * 3 + [vmem()] * 3,
        out_specs=vmem(),
        scratch_shapes=[
            buf(rows + WINDOW, 128),
            buf(rows + WINDOW, 128),
            buf(rows // WINDOW, HD, WINDOW),
            buf(tp_count * HD, chip_rows),
            buf(chip_rows, tp_count * HD),
            buf(nc, tp_count * HD, fc),
            buf(chip_rows, half),
            buf(chip_rows, half),
            buf(chip_rows, 128, dtype=f32),
            buf(chip_rows, 128, dtype=f32),
            buf(rows, experts),
            buf(experts, rows),
            buf(rows, experts),
            buf(slots, rows),
            buf(rows, slots),
            buf(tp_count // 2, 8, chip_rows, dtype=f32),
            buf(rows, 128, dtype=f32),
            buf(slots, 128, dtype=f32),
            buf(nc, rows, fc),
            buf(slots, half),
            buf(slots, half),
            buf(slots, half),
            buf(hidden_units, width),
            buf(hidden_units, width),
            buf(slots, hidden_units, dtype=f32),
            buf(slots, hidden_units, dtype=f32),
            buf(4 * units, half),
            buf(rows, 4 * units, dtype=f32),
            buf(rows, 4 * units, dtype=f32),
            buf(slots, hidden_units),
            buf(rows, 2 * units),
            buf(hidden_units, width),
            buf(slots, half),
            buf(slots, half),
            buf(slots, half),
            buf(slots, half),
            buf(2 * units, half),
            buf(rows, half, dtype=f32),
            buf(2, hops, chip_rows, half),
            buf(2, hops, chip_rows, half),
            buf(tp_count // 2 - 1, chip_rows, half // sum(CUTS) * CUTS[-1]),
            buf(tp_count // 2 - 1, chip_rows, half // sum(CUTS) * CUTS[-1]),
            buf(my_rows, half),
            buf(my_rows, half),
            pltpu.SemaphoreType.DMA((3,)),
            *sems(2),
            *sems(1),
            *sems(nc),
            *sems(nc, 2, hops),
            *sems(1),
            *sems(1),
            *sems(nc, 2, hops),
            *sems(nc),
            *sems(nc),
            *sems(3),
            *sems(1),
            *sems(cuts),
            *sems(cuts),
            *sems(cuts, 2, hops),
            *sems(cuts),
            *sems(1),
            *sems(tp_count // 2 - 1),
        ],
        compiler_params=pltpu.CompilerParams(
            collective_id=1, has_side_effects=True, vmem_limit_bytes=66_000_000
        ),
    )(queries, keys, values, sink, w_out, residual, gain, ids, weights, wg, wu, wd, sg, su, sd)


def body(
    queries,
    keys,
    values,
    sink_logits,
    w_out,
    residual,
    norm_gain,
    expert_ids,
    expert_weights,
    w_gate,
    w_up,
    w_down,
    shared_gate,
    shared_up,
    shared_down,
):
    return layer(
        queries.T,
        keys,
        values,
        sink_logits[:, None],
        w_out,
        residual,
        norm_gain[None, :],
        expert_ids.T,
        expert_weights.T,
        w_gate[0],
        w_up[0],
        w_down[0],
        shared_gate,
        shared_up,
        shared_down,
    )


def solution(mesh):
    return jax.shard_map(
        body,
        mesh=mesh,
        in_specs=(
            P("sp", "tp"),
            P("sp", None),
            P("sp", None),
            P("tp"),
            P("tp", None),
            P(("sp", "tp"), None),
            P(),
            P("sp", None),
            P("sp", None),
            P(("sp", "tp"), None, None),
            P(("sp", "tp"), None, None),
            P(("sp", "tp"), None, None),
            P("tp", None),
            P("tp", None),
            P("tp", None),
        ),
        out_specs=P(("sp", "tp"), None),
        check_vma=False,
    )
```

```python
import jax
import jax.numpy as jnp
from jax import lax
from jax.experimental import pallas as pl
from jax.experimental.pallas import tpu as pltpu
from jax.sharding import PartitionSpec as P

HD = 64
GROUP = 4
WINDOW = 128
TOPK = 4


MESH = pl.DeviceIdType.MESH
CHUNKS = 4
TALL = 512
FAR = True
CUTS = (2, 2, 2, 1, 1)
CAP = 64


def dot_nt(a, b):
    return lax.dot_general(a, b, (((1,), (1,)), ((), ())), preferred_element_type=jnp.float32)


def dot_nn(a, b):
    return jnp.dot(a, b, preferred_element_type=jnp.float32)


def rows_loop(total, step, fn):
    def one(i, carry):
        fn(pl.ds(pl.multiple_of(i * step, step), step))
        return carry

    lax.fori_loop(0, total // step, one, 0, unroll=total == 2 * step)


class Place:
    def __init__(self):
        self.sp_count = lax.axis_size("sp")
        self.tp_count = lax.axis_size("tp")
        self.s = lax.axis_index("sp")
        self.t = lax.axis_index("tp")
        self.c = self.t % 2
        self.z = self.t // 2
        self.nz = self.tp_count // 2
        self.partner = (self.s, self.t + 1 - 2 * self.c)
        self.right = (self.s, (self.t + 2) % self.tp_count)
        self.left = (self.s, (self.t + self.tp_count - 2) % self.tp_count)

    def peer(self, o):
        return ((self.s + o) % self.sp_count, self.t)

    def barrier(self):
        sem = pltpu.get_barrier_semaphore()

        def greet(count, device):
            def one(o, carry):
                pl.semaphore_signal(sem, inc=1, device_id=device(o), device_id_type=MESH)
                return carry

            lax.fori_loop(1, count, one, 0)

        greet(self.tp_count, lambda o: (self.s, (self.t + o) % self.tp_count))
        greet(self.sp_count, self.peer)
        pl.semaphore_wait(sem, self.tp_count + self.sp_count - 2)

    def steps(self, j):
        far, near = self.nz // 2, self.nz - 1 - self.nz // 2
        return (far, near) if j % 2 == 0 else (near, far)


def remote(src, dst, send_sem, recv_sem, device):
    return pltpu.make_async_remote_copy(
        src_ref=src, dst_ref=dst, send_sem=send_sem, recv_sem=recv_sem, device_id=device, device_id_type=MESH
    )


class RingGather:
    def __init__(self, p, buf, rows, send_sems, recv_sems):
        self.p, self.buf, self.rows = p, buf, rows
        self.ss, self.rs = send_sems, recv_sems

    def copy(self, j, way, k, shift):
        p = self.p
        origin = (p.z - shift if way == 0 else p.z + shift) + p.nz
        block = self.buf.at[j, pl.ds(pl.multiple_of(origin % p.nz * self.rows, self.rows), self.rows)]
        return remote(block, block, self.ss.at[j, way, k - 1], self.rs.at[j, way, k - 1], p.left if way else p.right)

    def send(self, j, k):
        for way in range(2):
            if k <= self.p.steps(j)[way]:
                self.copy(j, way, k, k - 1).start()

    def wait(self, j, k):
        for way in range(2):
            if k <= self.p.steps(j)[way]:
                self.copy(j, way, k, k).wait_recv()

    def drain(self, j):
        for way in range(2):
            for k in range(1, self.p.steps(j)[way] + 1):
                self.copy(j, way, k, k - 1).wait_send()


class Exchange:
    def __init__(self, p, src, dst, rows, spans, send_sems, recv_sems):
        self.p, self.src, self.dst, self.rows, self.spans = p, src, dst, rows, spans
        self.ss, self.rs = send_sems, recv_sems

    def block(self, index, j):
        return pl.ds(pl.multiple_of(index * self.rows, self.rows), self.rows), self.spans[j]

    def send(self, j):
        p = self.p

        def one(o, carry):
            peer = p.peer(o)
            remote(
                self.src.at[self.block(peer[0], j)],
                self.dst.at[self.block(p.s, j)],
                self.ss.at[j],
                self.rs.at[j],
                peer,
            ).start()
            return carry

        lax.fori_loop(1, p.sp_count, one, 0)
        self.dst[self.block(p.s, j)] = self.src[self.block(p.s, j)]

    def all_of(self, j):
        others = pl.ds(0, (self.p.sp_count - 1) * self.rows), self.spans[j]
        return remote(self.src.at[others], self.dst.at[others], self.ss.at[j], self.rs.at[j], self.p.peer(1))

    def wait(self, j):
        self.all_of(j).wait_recv()

    def drain(self, j):
        self.all_of(j).wait_send()


def iota(shape, axis):
    return lax.broadcasted_iota(jnp.int32, shape, axis)


def silu_times(gate, up):
    return (gate / (1.0 + jnp.exp(-gate)) * up).astype(jnp.bfloat16)


def layer_kernel(
    queries, keys, values, sink, w_out, residual, gain, ids, weights, wg_hbm, wu_hbm, wd_hbm, sg, su, sd,
    out,
    key_ext, value_ext, att, heads, heads_t, wide, res, after, square, square_other,
    rank_buf, rank_t, weight_buf, pick, blend, scale_rows, scale_cols, scale_slots,
    ring_buf, outgoing, own, other, wg, wu, gate_sum, up_sum, sgu, pre, pre_other, hidden, shared,
    wd, half_send, half_recv, total, held, sdh, part, red_send, red_recv, far_send, far_recv, row_send, row_recv,
    w_sem, k_send, k_recv, h_send, h_recv, x_send, x_recv, o_send, o_recv, r_send, r_recv, q_send, q_recv,
    g_send, g_recv, a_send, a_recv, f_send, f_recv, s_send, s_recv,
    d_send, d_recv, t_send, t_recv, b_send, b_recv, e_send, e_recv, m_send, m_recv, n_send, n_recv, z_send, z_recv,
):
    p = Place()
    c, nc = p.c, CHUNKS
    rows = queries.shape[1]
    my_rows, width = residual.shape
    half = width // 2
    fc = half // nc
    head_rows = w_out.shape[0]
    chip_rows = 2 * my_rows
    blocks = rows // WINDOW
    experts = p.sp_count * p.nz
    slots = pick.shape[0]
    capacity = slots // p.sp_count
    units = sg.shape[0]
    tile = min(256, rows, slots)
    tall = min(TALL, rows, slots)
    last = p.nz // 2
    everything = tuple(range(nc))
    kv = p.t // GROUP
    kv_cols = pl.ds(pl.multiple_of(kv // 2 * 128, 128), 128)
    f32, bf = jnp.float32, jnp.bfloat16

    def half_of(h):
        return pl.ds(pl.multiple_of(h * half, half), half)

    def cols(h, j):
        return pl.ds(pl.multiple_of(h * half + j * fc, fc), fc)

    pairs = ((wg_hbm, wg), (wu_hbm, wu), (wd_hbm, wd))
    fetches = [pltpu.make_async_copy(src, dst, w_sem.at[i]) for i, (src, dst) in enumerate(pairs)]
    for copy in fetches:
        copy.start()
    p.barrier()

    def shard(core):
        return pl.ds(pl.multiple_of(p.z * 2 * head_rows + core * head_rows, head_rows), head_rows)

    def swap(j, core):
        return remote(
            w_out.at[:, cols(1 - c, j)], wide.at[j, shard(core)], x_send.at[j], x_recv.at[j], p.partner
        )

    rim = pl.ds(rows - WINDOW, WINDOW)
    following = ((p.s + 1) % p.sp_count, p.t)
    halo = [
        remote(ref.at[rim, kv_cols], ext.at[pl.ds(0, WINDOW)], k_send.at[i], k_recv.at[i], following)
        for i, (ref, ext) in enumerate(((keys, key_ext), (values, value_ext)))
    ]
    sends_rim, gets_rim = p.s + 1 < p.sp_count, p.s > 0

    def part_of(core):
        return pl.ds(pl.multiple_of(core * my_rows, my_rows), my_rows)

    def swap_res(core):
        return remote(residual.at[:, half_of(1 - c)], res.at[part_of(core)], r_send.at[0], r_recv.at[0], p.partner)

    unit_rows = [pl.ds(pl.multiple_of(k * 2 * units + c * units, units), units) for k in range(2)]
    my_units = pl.ds(pl.multiple_of(c * units, units), units)
    shared_swaps = [
        remote(sg.at[:, half_of(1 - c)], sgu.at[unit_rows[0]], s_send.at[0], s_recv.at[0], p.partner),
        remote(su.at[:, half_of(1 - c)], sgu.at[unit_rows[1]], s_send.at[1], s_recv.at[1], p.partner),
        remote(sd.at[:, half_of(1 - c)], sdh.at[my_units], d_send.at[0], d_recv.at[0], p.partner),
    ]
    for j in everything:
        swap(j, c).start()

    @pl.when(sends_rim)
    def _():
        for copy in halo:
            copy.start()

    swap_res(c).start()
    for copy in shared_swaps:
        copy.start()
    for j in everything:
        wide[j, shard(c)] = w_out[:, cols(c, j)]
    ring = RingGather(p, wide, 2 * head_rows, o_send, o_recv)
    first, second = (0, 1), (2, 3)
    turns = sorted([(2 * k, first, k) for k in range(last)] + [(2 * k + 3, second, k) for k in range(last)])
    hops = [(j, k) for _, pair, k in turns for j in pair]

    def hop(count=1):
        for _ in range(min(count, len(hops))):
            j, k = hops.pop(0)
            if k:
                ring.wait(j, k)
            else:
                swap(j, 1 - c).wait_recv()
            ring.send(j, k + 1)

    hop(2)
    key_ext[pl.ds(WINDOW, rows)] = keys[:, kv_cols]
    value_ext[pl.ds(WINDOW, rows)] = values[:, kv_cols]
    res[part_of(c)] = residual[:, half_of(c)]
    sgu[unit_rows[0]] = sg[:, half_of(c)]
    sgu[unit_rows[1]] = su[:, half_of(c)]
    sdh[my_units] = sd[:, half_of(c)]

    @pl.when(gets_rim)
    def _():
        for copy in halo:
            copy.wait_recv()

    @pl.when(jnp.logical_not(gets_rim))
    def _():
        key_ext[pl.ds(0, WINDOW)] = jnp.zeros((WINDOW, 128), bf)
        value_ext[pl.ds(0, WINDOW)] = jnp.zeros((WINDOW, 128), bf)

    lane_half = kv % 2
    sink_value = sink[...]
    head_place = pl.ds(pl.multiple_of(p.t * HD, HD), HD)

    def head_piece(b, device):
        return remote(att.at[b], heads.at[head_place], h_send.at[0], h_recv.at[0], device)

    others = heads.at[pl.ds(0, (p.tp_count - 1) * HD)]
    head_total = remote(others, others, h_send.at[0], h_recv.at[0], p.partner)

    def attend(i):
        b = (p.z + i) % blocks
        here = pl.ds(pl.multiple_of(b * WINDOW, WINDOW), WINDOW)
        ext = pl.ds(pl.multiple_of(b * WINDOW, WINDOW), 2 * WINDOW)
        query = queries[:, here].astype(f32)
        query = jnp.concatenate([query, query], axis=0)
        in_half = jnp.right_shift(iota((2 * HD, WINDOW), 0), HD.bit_length() - 1) == lane_half
        query = jnp.where(in_half, query, 0.0).astype(bf)
        scores = dot_nn(key_ext[ext], query) * HD ** (-0.5)
        key_pos = iota((2 * WINDOW, WINDOW), 0)
        query_pos = iota((2 * WINDOW, WINDOW), 1) + WINDOW
        first_key = jnp.where(p.s * blocks + b == 0, WINDOW, 0)
        allowed = (key_pos <= query_pos) & (key_pos > query_pos - WINDOW) & (key_pos >= first_key)
        scores = jnp.where(allowed, scores, -jnp.inf)
        top = jnp.maximum(jnp.max(scores, axis=0, keepdims=True), sink_value)
        exps = jnp.exp(scores - top)
        full = jnp.sum(exps, axis=0, keepdims=True) + jnp.exp(sink_value - top)
        shares = (exps / full).astype(bf)
        both = lax.dot_general(
            value_ext[ext], shares, (((0,), (0,)), ((), ())), preferred_element_type=f32
        )
        att[b] = jnp.where(lane_half == 0, both[:HD], both[HD:]).astype(bf)
        for core in range(2):
            target = 2 * b + core

            @pl.when(target != p.t)
            def _():
                head_piece(b, (p.s, target)).start()

            @pl.when(target == p.t)
            def _():
                heads[head_place] = att[b]

    def attend_some(first, count):
        def one(i, carry):
            attend(i)
            return carry

        lax.fori_loop(first, first + count, one, 0)

    quarter = max(1, blocks // 4)
    for i in range(0, blocks, quarter):
        attend_some(i, quarter)
        hop((1, 3, 2, 2)[i // quarter])

    shift = capacity.bit_length() - 1

    def name_rows(i, carry):
        span = pl.ds(pl.multiple_of(i * tile, tile), tile)
        expert = iota((experts, tile), 0)
        named = jnp.zeros((experts, tile), f32)
        weight = jnp.zeros((experts, tile), f32)
        tile_ids, tile_weights = ids[:, span], weights[:, span]
        for k in range(TOPK):
            same = tile_ids[k : k + 1] == expert
            named = jnp.where(same, 1.0, named)
            weight = jnp.where(same, tile_weights[k : k + 1], weight)
        rank_t[:, span] = named.astype(bf)
        weight_buf[span] = weight.T.astype(bf)
        return carry

    lax.fori_loop(0, rows // tile, name_rows, 0)
    hop()
    all_named = rank_t[...]
    ranks = []
    for i in range(rows // tile):
        before = iota((rows, tile), 0) < iota((rows, tile), 1) + i * tile
        rank = dot_nn(all_named, jnp.where(before, 1.0, 0.0).astype(bf))
        named = all_named[:, i * tile : (i + 1) * tile].astype(f32) > 0.0
        ranks.append(jnp.where(named, rank, -1.0))
    for i, rank in enumerate(ranks):
        rank_t[:, i * tile : (i + 1) * tile] = rank.astype(bf)
        rank_buf[i * tile : (i + 1) * tile] = rank.T.astype(bf)
    hop()

    def holds(first, count):
        slot = iota((count, experts), 0) + first
        same = jnp.right_shift(slot, shift) * p.nz + p.z == iota((count, experts), 1)
        return jnp.where(same, 1.0, 0.0).astype(bf)

    def fill_pick(r, first):
        place = jnp.bitwise_and(iota((tile, rows), 0) + first, capacity - 1).astype(f32)
        hit = dot_nn(holds(first, tile), rank_t[...]) == place
        pick[r] = jnp.where(hit, 1.0, 0.0).astype(bf)

    for i in range(slots // tile):
        fill_pick(pl.ds(i * tile, tile), i * tile)
        hop()

    def fill_blend(r):
        all_holds = holds(0, slots)
        place = jnp.bitwise_and(iota((tile, slots), 1), capacity - 1).astype(f32)
        hit = dot_nt(rank_buf[r], all_holds) == place
        blend[r] = jnp.where(hit, dot_nt(weight_buf[r], all_holds), 0.0).astype(bf)

    def fill_blend_tiles(first, end):
        for i in range(first, end):
            fill_blend(pl.ds(i * tile, tile))

    hop(len(hops) - 2)

    head_total.wait_recv()
    heads_t[...] = heads[...].T
    swap_res(1 - c).wait_recv()
    chip_place = pl.ds(pl.multiple_of(p.z * chip_rows, chip_rows), chip_rows)
    gather = RingGather(p, ring_buf, chip_rows, g_send, g_recv)

    def project(j):
        ring.wait(j, last)
        piece = pl.ds(j * fc, fc)
        mixed = (res[:, piece].astype(f32) + dot_nn(heads_t[...], wide[j])).astype(bf)
        after[:, piece] = mixed
        ring_buf[j, chip_place] = mixed
        gather.send(j, 1)
        mixed = mixed.astype(f32)
        return jnp.sum(mixed * mixed, axis=1, keepdims=True)

    def pass_on(pair, k):
        for j in pair if k < last else ():
            gather.wait(j, k)
            gather.send(j, k + 1)

    squares = project(0) + project(1)
    hop(2)
    pass_on(first, 1)
    squares = squares + project(2) + project(3)
    square[...] = jnp.broadcast_to(squares, square.shape)
    swap_square = remote(square, square_other, q_send.at[0], q_recv.at[0], p.partner)
    swap_square.start()
    pass_on(first, 2)
    swap_square.wait_recv()
    mean = (square[...] + square_other[...]) / width
    scale_rows[p.z] = lax.rsqrt(mean + 1e-06).T[:8]

    def send_scale(o):
        mine = scale_rows.at[p.z]
        return remote(mine, mine, n_send.at[0], n_recv.at[0], (p.s, (p.t + 2 * o) % p.tp_count))

    for o in range(1, p.nz):
        send_scale(o).start()
    all_scales = scale_rows.at[pl.ds(0, p.nz - 1)]
    scale_total = remote(all_scales, all_scales, n_send.at[0], n_recv.at[0], p.partner)

    def take_scales():
        scale_total.wait_recv()
        for z in range(p.nz):
            block = jnp.broadcast_to(scale_rows[z, :1], (128, chip_rows))
            scale_cols[z * chip_rows : (z + 1) * chip_rows] = block.T
        flat = jnp.concatenate([scale_rows[z, :1] for z in range(p.nz)], axis=1)

        def one(r):
            found = jnp.sum(pick[r].astype(f32) * flat, axis=1, keepdims=True)
            scale_slots[r] = jnp.broadcast_to(found, (tile, 128))

        rows_loop(slots, tile, one)

    even = [pl.ds(j * fc, fc) for j in everything]
    spread = Exchange(p, outgoing, own, capacity, even, a_send, a_recv)

    def forward(j):
        return remote(own.at[:, even[j]], other.at[:, even[j]], f_send.at[j], f_recv.at[j], p.partner)

    def select(j):
        gather.wait(j, last)

        def one(r):
            value = dot_nn(pick[r], ring_buf[j]) * scale_slots[r][:, :1] * gain[:, cols(c, j)]
            outgoing[r, even[j]] = value.astype(bf)

        rows_loop(slots, tall, one)
        spread.send(j)

    def shared_part(j):
        def one(r):
            normed = ring_buf[j, r].astype(f32) * scale_cols[r][:, :1] * gain[:, cols(c, j)]
            value = dot_nt(normed.astype(bf), sgu[:, j * fc : (j + 1) * fc])
            pre[r] = value if j == 0 else pre[r] + value

        rows_loop(rows, tile, one)

    def arrive(j):
        spread.wait(j)
        forward(j).start()

    def multiply(j):
        forward(j).wait_recv()

        def one(r):
            both = jnp.concatenate([own[r, even[j]], other[r, even[j]]], axis=1)
            for w, acc in ((wg, gate_sum), (wu, up_sum)):
                across = jnp.concatenate([w[:, cols(c, j)], w[:, cols(1 - c, j)]], axis=1)
                value = dot_nt(both, across)
                acc[r] = value if j == 0 else acc[r] + value

        rows_loop(slots, tall, one)

    fill_blend_tiles(0, rows // tile)
    pass_on(second, 1)
    pass_on(first, 3)
    for copy in shared_swaps:
        copy.wait_recv()
    pass_on(second, 2)
    take_scales()
    select(0)
    pass_on(second, 3)
    for j in (1, 2, 3):
        select(j)
    for j in (0, 1):
        shared_part(j)
    arrive(0)
    for copy in fetches[:2]:
        copy.wait()
    multiply(0)
    for j in (2, 3):
        shared_part(j)
    swap_pre = remote(pre, pre_other, s_send.at[2], s_recv.at[2], p.partner)
    swap_pre.start()
    arrive(1)
    swap_pre.wait_recv()

    def shared_one(r):
        both = pre[r] + pre_other[r]
        shared[r] = silu_times(both[:, : 2 * units], both[:, 2 * units :])

    rows_loop(rows, tile, shared_one)
    multiply(1)
    arrive(2)
    multiply(2)
    arrive(3)
    multiply(3)

    def hidden_one(r):
        hidden[r] = silu_times(gate_sum[r], up_sum[r])

    rows_loop(slots, tile, hidden_one)

    fetches[2].wait()
    unit = half // sum(CUTS)
    starts = [sum(CUTS[:j]) * unit for j in range(len(CUTS))]
    sizes = [cut * unit for cut in CUTS]
    spans = [pl.ds(a, n) for a, n in zip(starts, sizes)]
    count = len(CUTS)
    direct = count - 1 if FAR else None
    back = Exchange(p, total, held, capacity, spans, b_send, b_recv)

    def span_of(h, j):
        return pl.ds(pl.multiple_of(h * half + starts[j], unit), sizes[j])

    def give(j):
        return remote(half_send.at[:, spans[j]], half_recv.at[:, spans[j]], t_send.at[j], t_recv.at[j], p.partner)

    def down(j):
        def theirs(r):
            half_send[r, spans[j]] = dot_nn(hidden[r], wd[:, span_of(1 - c, j)]).astype(bf)

        def ours(r):
            total[r, spans[j]] = dot_nn(hidden[r], wd[:, span_of(c, j)]).astype(bf)

        rows_loop(slots, tall, theirs)
        give(j).start()
        rows_loop(slots, tall, ours)

    def add_halves(j):
        give(j).wait_recv()

        def one(r):
            both = total[r, spans[j]].astype(f32) + half_recv[r, spans[j]].astype(f32)
            total[r, spans[j]] = both.astype(bf)

        rows_loop(slots, tile, one)
        back.send(j)

    def blend_rows(j):
        back.wait(j)

        def one(r):
            mixed = dot_nn(blend[r], held[:, spans[j]])
            part[r, spans[j]] = mixed + dot_nn(shared[r], sdh[:, spans[j]])

        rows_loop(rows, tall, one)

    def chip_block(distance):
        index = (p.z + distance + p.nz) % p.nz
        return pl.ds(pl.multiple_of(index * chip_rows, chip_rows), chip_rows)

    def red(j, way, m):
        sems = e_send.at[j, way, m - 1], e_recv.at[j, way, m - 1]
        refs = [ref.at[way, m - 1, :, spans[j]] for ref in (red_send, red_recv)]
        return remote(*refs, *sems, p.left if way else p.right)

    def step(j, m):
        for way in range(2):
            n = p.steps(j)[way]
            if m > n:
                continue
            distance = n - m + 1
            value = part[chip_block(-distance if way else distance), spans[j]]
            if m > 1:
                red(j, way, m - 1).wait_recv()
                value = value + red_recv[way, m - 2, :, spans[j]].astype(f32)
            red_send[way, m - 1, :, spans[j]] = value.astype(bf)
            red(j, way, m).start()

    def far(o):
        device = (p.s, (p.t + 2 * o) % p.tp_count)
        return remote(far_send.at[o - 1], far_recv.at[o - 1], z_send.at[o - 1], z_recv.at[o - 1], device)

    def send_far(j):
        for o in sorted(range(1, p.nz), key=lambda o: -min(o, p.nz - o)):
            far_send[o - 1] = part[chip_block(o), spans[j]].astype(bf)
            far(o).start()

    def give_rows(j):
        return remote(row_send.at[:, spans[j]], row_recv.at[:, spans[j]], m_send.at[j], m_recv.at[j], p.partner)

    def finish(j):
        ends = []
        if j == direct:
            for o in range(1, p.nz):
                far(o).wait_recv()
                ends.append(far_recv.at[o - 1])
        else:
            for way in range(2):
                n = p.steps(j)[way]
                if n:
                    red(j, way, n).wait_recv()
                    ends.append(red_recv.at[way, n - 1, :, spans[j]])

        def layer_rows(core):
            base = pl.ds(pl.multiple_of(p.z * chip_rows + core * my_rows, my_rows), my_rows)
            value = part[base, spans[j]]
            for end in ends:
                value = value + end[part_of(core)].astype(f32)
            moe = value.astype(bf).astype(f32)
            return (after[part_of(core), spans[j]].astype(f32) + moe).astype(bf)

        row_send[:, spans[j]] = layer_rows(1 - c)
        give_rows(j).start()
        out[:, span_of(c, j)] = layer_rows(c)

    def take_rows(j):
        give_rows(j).wait_recv()
        out[:, span_of(1 - c, j)] = row_recv[:, spans[j]]

    down(0)
    for j in range(1, count):
        down(j)
        add_halves(j - 1)
    add_halves(count - 1)
    at = {}

    def advance():
        for j in sorted(at):
            if j == direct:
                if at[j] == 1:
                    send_far(j)
                elif at[j] == last:
                    finish(j)
            elif at[j] <= last:
                step(j, at[j])
            elif at[j] == last + 1:
                finish(j)
            at[j] += 1

    for j in range(count):
        blend_rows(j)
        at[j] = 1
        advance()
    while any(at[j] <= last + (j != direct) for j in at):
        advance()
    for j in range(count):
        take_rows(j)

    @pl.when(sends_rim)
    def _():
        for copy in halo:
            copy.wait_send()

    for j in everything:
        swap(j, c).wait_send()
        ring.drain(j)
        gather.drain(j)
        spread.drain(j)
        forward(j).wait_send()
    swap_res(c).wait_send()
    head_total.wait_send()
    swap_square.wait_send()
    for copy in shared_swaps:
        copy.wait_send()
    swap_pre.wait_send()
    for j in range(count):
        give(j).wait_send()
        back.drain(j)
        give_rows(j).wait_send()
        for way in range(2):
            for m in range(1, p.steps(j)[way] + 1 if j != direct else 1):
                red(j, way, m).wait_send()
    scale_total.wait_send()
    for o in range(1, p.nz if FAR else 1):
        far(o).wait_send()


def vmem():
    return pl.BlockSpec(memory_space=pltpu.VMEM)


def layer(queries, keys, values, sink, w_out, residual, gain, ids, weights, wg, wu, wd, sg, su, sd):
    nc, cuts = CHUNKS, len(CUTS)
    rows = queries.shape[1]
    my_rows, width = residual.shape
    half, chip_rows = width // 2, 2 * my_rows
    fc = half // nc
    tp_count, sp_count = lax.axis_size("tp"), lax.axis_size("sp")
    experts = sp_count * tp_count // 2
    slots = sp_count * CAP
    hops = tp_count // 4
    hidden_units, units = wg.shape[0], sg.shape[0]
    bf, f32 = jnp.bfloat16, jnp.float32

    def buf(*shape, dtype=bf):
        return pltpu.VMEM(shape, dtype)

    def sems(*shape):
        return [pltpu.SemaphoreType.DMA(shape)] * 2

    anywhere = pl.BlockSpec(memory_space=pl.ANY)
    return pl.pallas_call(
        layer_kernel,
        name="layer",
        out_shape=jax.ShapeDtypeStruct((my_rows, width), bf),
        in_specs=[vmem()] * 9 + [anywhere] * 3 + [vmem()] * 3,
        out_specs=vmem(),
        scratch_shapes=[
            buf(rows + WINDOW, 128),
            buf(rows + WINDOW, 128),
            buf(rows // WINDOW, HD, WINDOW),
            buf(tp_count * HD, chip_rows),
            buf(chip_rows, tp_count * HD),
            buf(nc, tp_count * HD, fc),
            buf(chip_rows, half),
            buf(chip_rows, half),
            buf(chip_rows, 128, dtype=f32),
            buf(chip_rows, 128, dtype=f32),
            buf(rows, experts),
            buf(experts, rows),
            buf(rows, experts),
            buf(slots, rows),
            buf(rows, slots),
            buf(tp_count // 2, 8, chip_rows, dtype=f32),
            buf(rows, 128, dtype=f32),
            buf(slots, 128, dtype=f32),
            buf(nc, rows, fc),
            buf(slots, half),
            buf(slots, half),
            buf(slots, half),
            buf(hidden_units, width),
            buf(hidden_units, width),
            buf(slots, hidden_units, dtype=f32),
            buf(slots, hidden_units, dtype=f32),
            buf(4 * units, half),
            buf(rows, 4 * units, dtype=f32),
            buf(rows, 4 * units, dtype=f32),
            buf(slots, hidden_units),
            buf(rows, 2 * units),
            buf(hidden_units, width),
            buf(slots, half),
            buf(slots, half),
            buf(slots, half),
            buf(slots, half),
            buf(2 * units, half),
            buf(rows, half, dtype=f32),
            buf(2, hops, chip_rows, half),
            buf(2, hops, chip_rows, half),
            buf(tp_count // 2 - 1, chip_rows, half // sum(CUTS) * CUTS[-1]),
            buf(tp_count // 2 - 1, chip_rows, half // sum(CUTS) * CUTS[-1]),
            buf(my_rows, half),
            buf(my_rows, half),
            pltpu.SemaphoreType.DMA((3,)),
            *sems(2),
            *sems(1),
            *sems(nc),
            *sems(nc, 2, hops),
            *sems(1),
            *sems(1),
            *sems(nc, 2, hops),
            *sems(nc),
            *sems(nc),
            *sems(3),
            *sems(1),
            *sems(cuts),
            *sems(cuts),
            *sems(cuts, 2, hops),
            *sems(cuts),
            *sems(1),
            *sems(tp_count // 2 - 1),
        ],
        compiler_params=pltpu.CompilerParams(
            collective_id=1, has_side_effects=True, vmem_limit_bytes=66_000_000
        ),
    )(queries, keys, values, sink, w_out, residual, gain, ids, weights, wg, wu, wd, sg, su, sd)


def body(
    queries,
    keys,
    values,
    sink_logits,
    w_out,
    residual,
    norm_gain,
    expert_ids,
    expert_weights,
    w_gate,
    w_up,
    w_down,
    shared_gate,
    shared_up,
    shared_down,
):
    return layer(
        queries.T,
        keys,
        values,
        sink_logits[:, None],
        w_out,
        residual,
        norm_gain[None, :],
        expert_ids.T,
        expert_weights.T,
        w_gate[0],
        w_up[0],
        w_down[0],
        shared_gate,
        shared_up,
        shared_down,
    )


def solution(mesh):
    return jax.shard_map(
        body,
        mesh=mesh,
        in_specs=(
            P("sp", "tp"),
            P("sp", None),
            P("sp", None),
            P("tp"),
            P("tp", None),
            P(("sp", "tp"), None),
            P(),
            P("sp", None),
            P("sp", None),
            P(("sp", "tp"), None, None),
            P(("sp", "tp"), None, None),
            P(("sp", "tp"), None, None),
            P("tp", None),
            P("tp", None),
            P("tp", None),
        ),
        out_specs=P(("sp", "tp"), None),
        check_vma=False,
    )
```
